32 devices in a mesh: ep: 8 (over z, x), tp: 4 (over y, core).
Axes of the slice: x: 2, y: 2, z: 4, core: 2. Of those that a mesh axis runs over, the one named last changes fastest.
Arguments:
- tokens: bfloat16 [128, 2048], P('ep'), may hold values from -6 to 6
- lengths: int32 [128], P('ep'), may hold values from 1 to 1024, as said below
- key_cache: bfloat16 [128, 1024, 8, 128], P('ep', None, 'tp'), may hold values from -200 to 200
- value_cache: bfloat16 [128, 1024, 8, 128], P('ep', None, 'tp'), may hold values from -6 to 6
- attn_gain: float32 [2048], replicated, may hold values from 0.1 to 1.9
- w_query: bfloat16 [2048, 8, 128], P(None, 'tp'), may hold values from -0.1875 to 0.1875
- w_key: bfloat16 [2048, 8, 128], P(None, 'tp'), may hold values from -0.15625 to 0.15625
- w_value: bfloat16 [2048, 8, 128], P(None, 'tp'), may hold values from -0.125 to 0.125
- mix_lambda: float32 [8], P('tp'), may hold values from 0.3 to 0.8
- head_gain: float32 [128], replicated, may hold values from 0.1 to 1.9
- w_out: bfloat16 [8, 128, 2048], P('tp'), may hold values from -2.5 to 2.5
- ffn_gain: float32 [2048], replicated, may hold values from 0.1 to 1.9
- w_gate: bfloat16 [8, 2048, 2048], P('ep', None, 'tp'), may hold values from -1 to 1
- w_up: bfloat16 [8, 2048, 2048], P('ep', None, 'tp'), may hold values from -1 to 1
- w_down: bfloat16 [8, 2048, 2048], P('ep', 'tp'), may hold values from -0.046875 to 0.046875
- routes: int32 [128, 4], P('ep'), may hold values from 0 to 7, all different within a row; in each aligned block of 16 rows (0 to 15, 16 to 31, ...) at most 16 rows name the same one
- route_weights: float32 [128, 4], P('ep'), may hold values from 0.1 to 1
Outputs:
- mixed: bfloat16 [128, 2048], P('ep', 'tp')
The draws below stay inside these ranges and needn't reach their ends.
Inputs may be any that keep to these rules, and one draw needn't show every extreme that they name: `routes`: in each aligned block of 16 rows no expert is named by more than 16 entries, and one is named by exactly 16 in some block; each row names 4 different experts. `lengths`: some sequence has all 1024 positions valid.
All inputs are finite; a program needn't handle non-finite values.
Results may differ from the reference program's by a relative error of at most 0.02.
The reference program's roundings to bfloat16 on the way count: a program that leaves them out, or rounds other values in their place, can miss the bound.
Values may be sent and summed in bfloat16 or wider, within the bound.
A program may use at most 128 MiB of HBM per device.

```python
import math
import jax
import jax.numpy as jnp
import numpy as np
from jax import lax

D = 2048
HEADS = 8
HALF = 64
VDIM = 128
FF = 2048
TOP = 4
SEQ_DEV = 16
LEN = 1024
SEQS = 128
EXPERTS = 8
CAP = 16
GROUP_HEADS = 2
FF_DEV = 512
N_TP = 4


def draw_key_cache(key, part):
    base = jnp.clip(jax.random.normal(jax.random.fold_in(key, 11), (SEQS, LEN, HEADS, VDIM), jnp.float32), -6.0, 6.0)
    return base.astype(jnp.bfloat16)


def draw_lengths(key, part):
    groups = SEQS // SEQ_DEV
    limits = jax.random.randint(jax.random.fold_in(key, 21), (groups,), LEN // 8, LEN + 1)
    fullest = jax.random.randint(jax.random.fold_in(key, 22), (), 0, groups)
    group_ids = lax.iota(jnp.int32, groups)
    limits = jnp.where(group_ids == fullest, LEN, limits)
    raw_bits = jax.random.randint(jax.random.fold_in(key, 23), (groups, SEQ_DEV), 0, 1 << 30)
    seq_lengths = raw_bits % limits[:, None] + 1
    chosen_seq = jax.random.randint(jax.random.fold_in(key, 24), (), 0, SEQ_DEV)
    hit = (group_ids[:, None] == fullest) & (lax.iota(jnp.int32, SEQ_DEV)[None, :] == chosen_seq)
    seq_lengths = jnp.where(hit, LEN, seq_lengths)
    return seq_lengths.reshape(SEQS).astype(jnp.int32)


def shard_levels(own_key, shape, cuts, smallest, high):
    factor_of, own = 1.0, jax.random.fold_in(own_key, 6)
    for axis_at, shards_of in cuts:
        draws = jnp.exp(jax.random.uniform(jax.random.fold_in(own, axis_at), (shards_of,), jnp.float32, smallest / len(cuts), high / len(cuts)))
        factor_of = factor_of * jnp.repeat(draws, shape[axis_at] // shards_of).reshape([-1 if axis == axis_at else 1 for axis in range(len(shape))])
    return factor_of


def routed_block(stream_key, own, number, rows, count, top, bound, lean):
    order = jax.random.permutation(stream_key, count)
    heavy_load, usual = portions_of(count, rows * top, bound, lean, True), portions_of(count, rows * top, bound, lean, False)
    places = jnp.arange(count)

    def named(sizes, rotation):
        used = int((sizes > 0).sum())
        fixed = max(1, used // 4)
        moved = fixed + (places - fixed + rotation * (used - fixed)) % max(1, count - fixed)
        return jnp.zeros((count,), jnp.int32).at[order[jnp.where(places < fixed, places, moved)]].set(jnp.asarray(sizes, jnp.int32))

    sizes = jnp.where(number % 4 == 0, named(heavy_load, number // 4), named(usual, number - number // 4 - 1))
    mixed = jax.random.permutation(jax.random.fold_in(own, 3), count)
    source_of, receiver = mixed[0:count // 2 * 2:2], mixed[1:count // 2 * 2:2]
    room = jnp.minimum(sizes[source_of] - 1, bound - sizes[receiver]) // 2
    room = jnp.where((source_of == order[0]) | (receiver == order[0]) | (sizes[receiver] == 0), 0, jnp.maximum(room, 0))
    moved = jax.random.randint(jax.random.fold_in(own, 4), (count // 2,), 0, 1 << 20) % (room + 1)
    sizes = sizes.at[source_of].add(-moved).at[receiver].add(moved)
    members = jnp.searchsorted(jnp.cumsum(sizes), jnp.arange(rows * top), side="right").astype(jnp.int32)
    grid = members.reshape(top, rows).T
    grid = grid[jax.random.permutation(jax.random.fold_in(own, 1), rows)]
    rotation = jax.random.randint(jax.random.fold_in(own, 2), (rows, 1), 0, top)
    return jnp.take_along_axis(grid, (jnp.arange(top)[None, :] + rotation) % top, axis=1)


def portions_of(count, total, bound, slope, full):
    loads = [(1 << 20) // math.isqrt(rank ** slope) + 1 for rank in range(1, count + 1)]
    largest = bound if full else min(bound, max(-(-total // count), total * loads[0] // sum(loads)))
    least = 1 if total - largest >= count - 1 else 0
    holding, spare = [largest] + [least] * (count - 1), total - largest - least * (count - 1)
    while spare > 0:
        free = [i for i in range(1, count) if holding[i] < largest] or [i for i in range(1, count) if holding[i] < bound]
        pool, left = sum([loads[i] for i in free]), spare
        for i in free:
            more = min(bound - holding[i], max(1, left * loads[i] // pool), spare)
            holding[i] = holding[i] + more
            spare = spare - more
    return np.array(holding)


def centred(rng, shape, spread, most, cuts=(), dtype=jnp.bfloat16):
    loudness = shard_levels(rng, shape, cuts, -0.22, 0.18) if cuts else 1.0
    array = jax.random.normal(rng, shape, jnp.float32) * spread * loudness
    return jnp.minimum(jnp.maximum(array, -most), most).astype(dtype)


def setup_inputs(seed: int = 0) -> dict:
    key_of = jax.random.split(jax.random.key(seed), 18)
    tokens = centred(key_of[0], (SEQS, D), 1.0, 6.0, ((0, 8),))
    lengths = draw_lengths(jax.random.fold_in(key_of[17], 71), 0)
    key_cache = draw_key_cache(jax.random.fold_in(key_of[17], 71), 0)
    value_cache = centred(key_of[3], (SEQS, LEN, HEADS, VDIM), 1.0, 6.0, ((0, 8), (2, 4)))
    attn_gain = jnp.clip(1.0 + 0.18 * jax.random.normal(key_of[4], (D,), jnp.float32), 0.1, 1.9)
    w_query = centred(key_of[5], (D, HEADS, VDIM), (D // 2) ** -0.5, 0.1875, ((1, 4),))
    w_key = centred(key_of[6], (D, HEADS, VDIM), (D * 2 // 3) ** -0.5, 0.15625, ((1, 4),))
    w_value = centred(key_of[7], (D, HEADS, VDIM), D ** -0.5, 0.125, ((1, 4),))
    mix_lambda = jnp.clip(0.3 + 0.5 * jax.random.uniform(key_of[8], (HEADS,), jnp.float32) ** shard_levels(key_of[8], (HEADS,), ((0, 4),), -0.2, 0.2), 0.3, 0.8)
    head_gain = jnp.clip(1.0 + 0.18 * jax.random.normal(key_of[9], (VDIM,), jnp.float32), 0.1, 1.9)
    w_out = centred(key_of[10], (HEADS, VDIM, D), (5.0 / (HEADS * VDIM) ** 0.5), 2.5, ((0, 4),))
    ffn_gain = jnp.clip(1.0 + 0.18 * jax.random.normal(key_of[11], (D,), jnp.float32), 0.1, 1.9)
    w_gate = centred(key_of[12], (EXPERTS, D, FF), (3.0 / D ** 0.5), 1.0, ((0, 8), (2, 4)))
    w_up = centred(key_of[13], (EXPERTS, D, FF), (3.0 / D ** 0.5), 1.0, ((0, 8), (2, 4)))
    w_down = centred(key_of[14], (EXPERTS, FF, D), (0.15 / FF ** 0.5), 0.046875, ((0, 8), (1, 4)))
    routes_keys = jax.random.split(jax.random.fold_in(key_of[15], 1), SEQS // SEQ_DEV)
    routes_turns = jax.random.permutation(jax.random.fold_in(key_of[15], 3), SEQS // SEQ_DEV)
    routes = jax.vmap(lambda own, number: routed_block(jax.random.fold_in(key_of[15], 2), own, number, SEQ_DEV, EXPERTS, TOP, CAP, 2))(routes_keys, routes_turns).reshape((SEQS, TOP))
    route_weights = jnp.clip(0.1 + 0.9 * jax.random.uniform(key_of[16], (SEQS, TOP), jnp.float32) ** shard_levels(key_of[16], (SEQS, TOP), ((0, 8),), -0.2, 0.2), 0.1, 1.0)
    return dict(tokens=tokens, lengths=lengths, key_cache=key_cache, value_cache=value_cache, attn_gain=attn_gain, w_query=w_query, w_key=w_key, w_value=w_value, mix_lambda=mix_lambda, head_gain=head_gain, w_out=w_out, ffn_gain=ffn_gain, w_gate=w_gate, w_up=w_up, w_down=w_down, routes=routes, route_weights=route_weights)


epsilon = 1e-06
clamp_limit = 7.0
sigmoid_slope = 1.702
branch_scale = 0.2

def norm_rows(source, gain):
    wide = source.astype(jnp.float32)
    return wide * lax.rsqrt(lax.optimization_barrier(jnp.mean(wide * wide, axis=-1, keepdims=True)) + epsilon) * gain

def reference(tokens, lengths, key_cache, value_cache, attn_gain, w_query, w_key, w_value, mix_lambda, head_gain, w_out, ffn_gain, w_gate, w_up, w_down, routes, route_weights):
    groups = SEQS // SEQ_DEV
    columns = HEADS * VDIM
    normed = norm_rows(tokens, attn_gain).astype(jnp.bfloat16)
    queries = jnp.dot(normed, w_query.reshape(D, columns), preferred_element_type=jnp.float32).astype(jnp.bfloat16)
    key_new = jnp.dot(normed, w_key.reshape(D, columns), preferred_element_type=jnp.float32).astype(jnp.bfloat16)
    value_new = jnp.dot(normed, w_value.reshape(D, columns), preferred_element_type=jnp.float32).astype(jnp.bfloat16)
    halves = (lax.iota(jnp.int32, VDIM) < HALF).astype(jnp.float32)
    selector = jnp.stack([halves, 1.0 - halves])
    score_scale = HALF ** (-0.5)
    positions = lax.iota(jnp.int32, LEN)

    def attend(blocks):
        query_rows, fresh_keys, fresh_values, key_rows, value_rows, seq_lengths = blocks
        query_wide = query_rows.astype(jnp.float32)[:, :, None, :] * selector[None, None]
        scores = jnp.einsum('shcd,slhd->shcl', query_wide, key_rows.astype(jnp.float32)) * score_scale
        own_scores = jnp.einsum('shcd,shd->shc', query_wide, fresh_keys.astype(jnp.float32)) * score_scale
        live_mask = (positions[None, :] < seq_lengths[:, None])[:, None, None, :]
        scores = jnp.where(live_mask, scores, -jnp.inf)
        peak = jnp.maximum(lax.optimization_barrier(jnp.max(scores, axis=-1)), own_scores)
        weights = jnp.exp(scores - peak[..., None])
        own_weight = jnp.exp(own_scores - peak)
        denominator = lax.optimization_barrier(jnp.sum(weights, axis=-1)) + own_weight
        shares = weights / denominator[..., None]
        own_share = own_weight / denominator
        balance = mix_lambda[None, :]
        mix_weights = (shares[:, :, 0] - balance[..., None] * shares[:, :, 1]).astype(jnp.bfloat16)
        own_mixed = (own_share[:, :, 0] - balance * own_share[:, :, 1]).astype(jnp.bfloat16)
        output = jnp.einsum('shl,slhd->shd', mix_weights.astype(jnp.float32), value_rows.astype(jnp.float32))
        return output + own_mixed.astype(jnp.float32)[..., None] * fresh_values.astype(jnp.float32)
    grouped = lax.map(attend, (queries.reshape(groups, SEQ_DEV, HEADS, VDIM), key_new.reshape(groups, SEQ_DEV, HEADS, VDIM), value_new.reshape(groups, SEQ_DEV, HEADS, VDIM), key_cache.reshape(groups, SEQ_DEV, LEN, HEADS, VDIM), value_cache.reshape(groups, SEQ_DEV, LEN, HEADS, VDIM), lengths.reshape(groups, SEQ_DEV)))
    heads_out = grouped.reshape(SEQS, HEADS, VDIM)
    normed_heads = (heads_out * lax.rsqrt(lax.optimization_barrier(jnp.mean(heads_out * heads_out, axis=-1, keepdims=True)) + epsilon) * head_gain * branch_scale).astype(jnp.bfloat16)
    parts = jnp.einsum('sgk,gkd->sgd', normed_heads.reshape(SEQS, N_TP, GROUP_HEADS * VDIM).astype(jnp.float32), w_out.reshape(N_TP, GROUP_HEADS * VDIM, D).astype(jnp.float32))
    attention = lax.optimization_barrier(jnp.sum(lax.optimization_barrier(parts.astype(jnp.bfloat16)).astype(jnp.float32), axis=1))
    residual = (tokens.astype(jnp.float32) + attention).astype(jnp.bfloat16)
    normed_ffn = norm_rows(residual, ffn_gain).astype(jnp.bfloat16)
    entries = routes.reshape(groups, SEQ_DEV * TOP)
    onehot = (entries[..., None] == lax.iota(jnp.int32, EXPERTS)[None, None, :]).astype(jnp.int32)
    entry_slot = lax.optimization_barrier(jnp.sum((jnp.cumsum(onehot, axis=1) - onehot) * onehot, axis=-1))
    target = (entries * CAP + entry_slot).astype(jnp.int32)
    placing = (lax.iota(jnp.int32, EXPERTS * CAP)[None, :, None] == target[:, None, :]).astype(jnp.float32)
    repeated = jnp.repeat(normed_ffn.reshape(groups, SEQ_DEV, D), TOP, axis=1).astype(jnp.float32)
    outgoing = jnp.einsum('gtr,grd->gtd', placing, repeated).astype(jnp.bfloat16)
    by_expert = outgoing.reshape(groups, EXPERTS, CAP, D).transpose(1, 0, 2, 3).reshape(EXPERTS, groups * CAP, D)

    def expert(blocks):
        arrived, gate_weight, up_weight, down_weight = blocks
        gate_value = jnp.minimum(jnp.dot(arrived, gate_weight, preferred_element_type=jnp.float32), clamp_limit)
        up_value = jnp.clip(jnp.dot(arrived, up_weight, preferred_element_type=jnp.float32), -clamp_limit, clamp_limit)
        activated = ((up_value + 1.0) * gate_value * jax.nn.sigmoid(sigmoid_slope * gate_value)).astype(jnp.bfloat16)
        pieces = jnp.einsum('rgf,gfd->rgd', activated.reshape(-1, N_TP, FF_DEV).astype(jnp.float32), down_weight.reshape(N_TP, FF_DEV, D).astype(jnp.float32))
        summed = lax.optimization_barrier(jnp.sum(lax.optimization_barrier(pieces.astype(jnp.bfloat16)).astype(jnp.float32), axis=1))
        return summed.astype(jnp.bfloat16)
    results = lax.map(expert, (by_expert, w_gate, w_up, w_down))
    returned = results.reshape(EXPERTS, groups, CAP, D).transpose(1, 0, 2, 3).reshape(groups, EXPERTS * CAP, D)
    chosen = (lax.iota(jnp.int32, EXPERTS * CAP)[None, None, None, :] == target.reshape(groups, SEQ_DEV, TOP)[..., None]).astype(jnp.float32)
    combine = lax.optimization_barrier(jnp.sum(route_weights.reshape(groups, SEQ_DEV, TOP, 1) * chosen, axis=2))
    expert_sum = jnp.einsum('gsr,grd->gsd', combine, returned.astype(jnp.float32), precision=lax.Precision.HIGHEST)
    return (residual.astype(jnp.float32) + expert_sum.reshape(SEQS, D)).astype(jnp.bfloat16)
```

```python
import functools

import jax
import jax.numpy as jnp
from jax import lax
from jax.experimental import pallas as pl
from jax.experimental.pallas import tpu as pltpu
from jax.sharding import PartitionSpec as P

epsilon = 1e-06
clamp_limit = 7.0
sigmoid_slope = 1.702
branch_scale = 0.2
MESH = pl.DeviceIdType.MESH
f32, bf16 = jnp.float32, jnp.bfloat16
lane_tile = 128
wide_tile = 256
key_chunks = 4


def norm_rows(wide, gain):
    return wide * lax.rsqrt(jnp.mean(wide * wide, axis=-1, keepdims=True) + epsilon) * gain


def dot(left, right):
    return jnp.dot(left, right, preferred_element_type=f32)


def dot_rows(left, right):
    return lax.dot_general(left, right, (((1,), (1,)), ((), ())), preferred_element_type=f32)


def iota(shape, axis):
    return lax.broadcasted_iota(jnp.int32, shape, axis)


def to_column(row):
    size = row.shape[1]
    eye = iota((size, size), 0) == iota((size, size), 1)
    return jnp.sum(jnp.where(eye, row, jnp.zeros_like(row)), axis=1, keepdims=True)


def layer_kernel(
    n_ep,
    n_tp,
    n_x,
    group_heads,
    lengths_hbm,
    lambda_hbm,
    tokens_hbm,
    attn_gain_hbm,
    head_gain_hbm,
    ffn_gain_hbm,
    routes_hbm,
    route_weights_hbm,
    w_query_hbm,
    w_key_hbm,
    w_value_hbm,
    key_hbm,
    value_hbm,
    w_out_hbm,
    w_gate_hbm,
    w_up_hbm,
    w_down_hbm,
    out_ref,
    lengths_ref,
    lambda_ref,
    tokens_ref,
    attn_gain_ref,
    head_gain_ref,
    ffn_gain_ref,
    routes_ref,
    route_weights_ref,
    w_query_ref,
    w_key_ref,
    w_value_ref,
    key_ref,
    value_ref,
    w_out_ref,
    w_gate_ref,
    w_up_ref,
    w_down_ref,
    query_ref,
    score_ref,
    mix_ref,
    part_ref,
    part_in_ref,
    rows_ref,
    normed_ref,
    piece_ref,
    piece_in_ref,
    back_ref,
    back_in_ref,
    load_sems,
    key_sems,
    value_sems,
    part_sems,
    rows_sems,
    pair_sems,
    piece_sems,
    back_sems,
    sent_sems,
):
    my_ep, my_tp = lax.axis_index("ep"), lax.axis_index("tp")
    n_core = 2 if n_tp % 2 == 0 else 1
    n_y = n_tp // n_core
    n_z = n_ep // n_x
    my_y, my_core = my_tp // n_core, lax.rem(my_tp, n_core)
    my_z, my_x = my_ep // n_x, lax.rem(my_ep, n_x)
    seq_dev, model_width = tokens_ref.shape
    flat_len, head_width = key_ref.shape[1:]
    half_width = head_width // 2
    block = out_ref.shape[1]

    singles = (
        (tokens_hbm, tokens_ref),
        (attn_gain_hbm, attn_gain_ref),
        (w_query_hbm, w_query_ref),
        (w_key_hbm, w_key_ref),
        (w_value_hbm, w_value_ref),
        (lengths_hbm, lengths_ref),
        (lambda_hbm, lambda_ref),
        (head_gain_hbm, head_gain_ref),
        (ffn_gain_hbm, ffn_gain_ref),
        (routes_hbm, routes_ref),
        (route_weights_hbm, route_weights_ref),
        (w_out_hbm, w_out_ref),
        (w_gate_hbm, w_gate_ref),
        (w_up_hbm, w_up_ref),
        (w_down_hbm, w_down_ref),
    )
    loads = [
        pltpu.make_async_copy(source, target, load_sems.at[i])
        for i, (source, target) in enumerate(singles)
    ]
    chunk = flat_len // key_chunks
    key_loads = [
        pltpu.make_async_copy(
            key_hbm.at[:, pl.ds(j * chunk, chunk), :],
            key_ref.at[:, pl.ds(j * chunk, chunk), :],
            key_sems.at[j],
        )
        for j in range(key_chunks)
    ]
    pairs = seq_dev // 2
    value_loads = [
        pltpu.make_async_copy(
            value_hbm.at[pl.ds(2 * i, 2)], value_ref.at[pl.ds(2 * i, 2)], value_sems.at[i]
        )
        for i in range(pairs)
    ]
    for copy in loads[:11] + key_loads + value_loads + loads[11:]:
        copy.start()

    def device(dz, dx, dy, dc):
        ep = lax.rem(my_z + dz, n_z) * n_x + lax.rem(my_x + dx, n_x)
        tp = lax.rem(my_y + dy, n_y) * n_core + lax.rem(my_core + dc, n_core)
        return ep, tp

    def source(dz, dx, dy, dc):
        return device(n_z - dz, n_x - dx, n_y - dy, n_core - dc)

    def distance(place):
        dz, dx, dy = place
        return min(dz, n_z - dz) + min(dx, n_x - dx) + min(dy, n_y - dy)

    places = [(dz, dx, dy) for dz in range(n_z) for dx in range(n_x) for dy in range(n_y)]
    places = sorted(places, key=lambda place: -distance(place))
    remote = places[:-1]
    near_first = places[::-1]
    number = lambda place: (place[0] * n_x + place[1]) * n_y + place[2]
    tp_peers = [(dy, dc) for dy in range(n_y) for dc in range(n_core)][1:]

    barrier = pltpu.get_barrier_semaphore()
    greeted = [place + (0,) for place in remote]
    greeted += [(0, 0, dy, dc) for dy, dc in tp_peers if dc]
    for place in greeted:
        pl.semaphore_signal(barrier, inc=1, device_id=device(*place), device_id_type=MESH)

    loads[0].wait()
    loads[1].wait()
    normed = norm_rows(tokens_ref[...].astype(f32), attn_gain_ref[...]).astype(bf16)
    span = wide_tile * group_heads
    blocks = model_width // wide_tile
    stacked = jnp.concatenate(
        [normed[:, b * wide_tile : (b + 1) * wide_tile] for b in range(blocks)], axis=0
    )
    if group_heads > 1:
        spread = iota((wide_tile, span), 1) // group_heads == iota((wide_tile, span), 0)
        stacked = dot(stacked, spread.astype(f32).astype(bf16))
    else:
        stacked = stacked.astype(f32)
    lane_head = lax.rem(iota((1, span), 1), group_heads)
    left = jnp.concatenate(
        [
            jnp.concatenate(
                [
                    jnp.where(
                        lane_head == h, stacked[b * seq_dev : (b + 1) * seq_dev], 0.0
                    ).astype(bf16)
                    for h in range(group_heads)
                ],
                axis=0,
            )
            for b in range(blocks)
        ],
        axis=1,
    )
    loads[2].wait()
    queries = dot(left, w_query_ref[...]).astype(bf16).astype(f32)
    loads[3].wait()
    key_new = dot(left, w_key_ref[...]).astype(bf16).astype(f32)
    loads[4].wait()
    value_new = dot(left, w_value_ref[...]).astype(bf16).astype(f32)

    score_scale = half_width ** (-0.5)
    group_rows = group_heads * seq_dev
    first_half = iota((1, head_width), 1) < half_width
    halves = jnp.concatenate(
        [jnp.where(first_half, queries, 0.0), jnp.where(first_half, 0.0, queries)], axis=0
    )
    own = jnp.sum(halves * jnp.concatenate([key_new, key_new], axis=0), axis=-1, keepdims=True)
    own = own * score_scale
    row_seq = lax.rem(iota((2 * group_rows, 1), 0), seq_dev)
    row_head = lax.rem(iota((2 * group_rows, 1), 0) // seq_dev, group_heads)
    for s in range(seq_dev):
        query_ref[:, s * head_width : (s + 1) * head_width] = jnp.where(
            row_seq == s, halves, 0.0
        ).astype(bf16)

    for load in loads[5:11]:
        load.wait()
    limit = to_column(lengths_ref[...]) * group_heads
    limit = jnp.concatenate([limit] * (2 * group_heads), axis=0)
    balance = jnp.concatenate(
        [jnp.broadcast_to(lambda_ref[0:1, h : h + 1], (seq_dev, 1)) for h in range(group_heads)],
        axis=0,
    )

    peak = own
    for j in range(key_chunks):
        key_loads[j].wait()
        keys = jnp.concatenate(
            [key_ref[s, j * chunk : (j + 1) * chunk, :] for s in range(seq_dev)], axis=1
        )
        scores = dot_rows(query_ref[...], keys) * score_scale
        column = iota((1, chunk), 1) + j * chunk
        live = (column < limit) & (lax.rem(column, group_heads) == row_head)
        scores = jnp.where(live, scores, -jnp.inf)
        score_ref[:, j * chunk : (j + 1) * chunk] = scores
        peak = jnp.maximum(peak, jnp.max(scores, axis=-1, keepdims=True))
    own_weight = jnp.exp(own - peak)
    denominator = own_weight
    for j in range(key_chunks):
        weights = jnp.exp(score_ref[:, j * chunk : (j + 1) * chunk] - peak)
        score_ref[:, j * chunk : (j + 1) * chunk] = weights
        denominator = denominator + jnp.sum(weights, axis=-1, keepdims=True)
    inverse = 1.0 / denominator
    own_share = own_weight * inverse
    own_mix = own_share[:group_rows] - balance * own_share[group_rows:]
    own_mix = own_mix.astype(bf16).astype(f32)
    minuend, subtrahend = inverse[:group_rows], balance * inverse[group_rows:]
    for j in range(key_chunks):
        columns = slice(j * chunk, (j + 1) * chunk)
        mix_ref[:, columns] = (
            score_ref[:group_rows, columns] * minuend - score_ref[group_rows:, columns] * subtrahend
        ).astype(bf16)

    heads_out = own_mix * value_new
    group_seq = row_seq[:group_rows]
    for i in range(pairs):
        value_loads[i].wait()
        both = dot(
            mix_ref[...], jnp.concatenate([value_ref[2 * i], value_ref[2 * i + 1]], axis=1)
        )
        heads_out = heads_out + jnp.where(group_seq == 2 * i, both[:, :head_width], 0.0)
        heads_out = heads_out + jnp.where(group_seq == 2 * i + 1, both[:, head_width:], 0.0)
    heads = norm_rows(heads_out, head_gain_ref[...] * branch_scale).astype(bf16)
    heads = jnp.concatenate(
        [heads[h * seq_dev : (h + 1) * seq_dev] for h in range(group_heads)], axis=1
    )

    loads[11].wait()
    for t in range(n_tp):
        part_ref[t] = dot(heads, w_out_ref[:, t * block : (t + 1) * block]).astype(bf16)
    pl.semaphore_wait(barrier, len(greeted))

    def column_block(tp):
        return pl.ds(pl.multiple_of(tp * block, block), block)

    def row_block(ep):
        return pl.ds(pl.multiple_of(ep * seq_dev, seq_dev), seq_dev)

    for i, (dy, dc) in enumerate(tp_peers):
        peer = device(0, 0, dy, dc)
        pltpu.make_async_remote_copy(
            src_ref=part_ref.at[peer[1]],
            dst_ref=part_in_ref.at[i],
            send_sem=sent_sems.at[0],
            recv_sem=part_sems.at[0],
            device_id=peer,
            device_id_type=MESH,
        ).start()
    own_columns, own_rows = column_block(my_tp), row_block(my_ep)
    attention = part_ref[my_tp].astype(f32)
    if tp_peers:
        pltpu.make_async_copy(part_in_ref, part_in_ref, part_sems.at[0]).wait()
        for i in range(len(tp_peers)):
            attention += part_in_ref[i].astype(f32)
    residual = (tokens_ref[:, own_columns].astype(f32) + attention).astype(bf16)
    rows_ref[own_rows, own_columns] = residual

    def rows_copy(owner, peer, send, recv):
        place = rows_ref.at[row_block(owner[0]), column_block(owner[1])]
        return pltpu.make_async_remote_copy(
            src_ref=place,
            dst_ref=place,
            send_sem=send,
            recv_sem=recv,
            device_id=peer,
            device_id_type=MESH,
        )

    me = (my_ep, my_tp)
    sibling = device(0, 0, 0, 1)
    for place in remote:
        rows_copy(me, device(*place, 0), sent_sems.at[1], rows_sems.at[number(place)]).start()
    for place in near_first:
        owner = source(*place, 0)
        if place != (0, 0, 0):
            rows_copy(owner, me, sent_sems.at[1], rows_sems.at[number(place)]).wait_recv()
        if n_core > 1:
            rows_copy(owner, sibling, sent_sems.at[2], pair_sems.at[0]).start()
    if n_core > 1:
        pltpu.make_async_copy(piece_in_ref, piece_in_ref, pair_sems.at[0]).wait()

    normed_ref[...] = norm_rows(rows_ref[...].astype(f32), ffn_gain_ref[...]).astype(bf16)
    loads[12].wait()
    gate_value = jnp.minimum(dot(normed_ref[...], w_gate_ref[...]), clamp_limit)
    loads[13].wait()
    up_value = jnp.clip(dot(normed_ref[...], w_up_ref[...]), -clamp_limit, clamp_limit)
    activated = (
        (up_value + 1.0) * gate_value * jax.nn.sigmoid(sigmoid_slope * gate_value)
    ).astype(bf16)
    loads[14].wait()

    far_y = sorted(range(n_y), key=lambda dy: -min(dy, n_y - dy))
    if n_core > 1:
        for dy in far_y:
            tp = device(0, 0, dy, 1)[1]
            piece = dot(activated, w_down_ref[:, column_block(tp)]).astype(bf16)
            piece_ref[dy] = piece.reshape(n_ep, seq_dev, block)
            pltpu.make_async_remote_copy(
                src_ref=piece_ref.at[dy],
                dst_ref=piece_in_ref.at[dy],
                send_sem=sent_sems.at[3],
                recv_sem=piece_sems.at[dy],
                device_id=sibling,
                device_id_type=MESH,
            ).start()
    for dy in far_y:
        tp = device(0, 0, dy, 0)[1]
        piece = dot(activated, w_down_ref[:, column_block(tp)]).reshape(n_ep, seq_dev, block)
        if n_core > 1:
            landed = piece_in_ref.at[dy]
            pltpu.make_async_copy(landed, landed, piece_sems.at[dy]).wait()
            piece = piece + piece_in_ref[dy].astype(f32)
        back_ref[dy] = piece.astype(bf16)
        for place in remote:
            if place[2] == dy:
                peer = device(*place, 0)
                pltpu.make_async_remote_copy(
                    src_ref=back_ref.at[dy, peer[0]],
                    dst_ref=back_in_ref.at[number(place) - 1],
                    send_sem=sent_sems.at[4],
                    recv_sem=back_sems.at[number(place)],
                    device_id=peer,
                    device_id_type=MESH,
                ).start()

    total = rows_ref[own_rows, own_columns].astype(f32)
    pending = {}
    for place in near_first:
        dz, dx, dy = place
        expert = source(*place, 0)[0]
        if place == (0, 0, 0):
            value = back_ref[0, my_ep].astype(f32)
        else:
            arrived = back_in_ref.at[number(place) - 1]
            pltpu.make_async_copy(arrived, arrived, back_sems.at[number(place)]).wait()
            value = back_in_ref[number(place) - 1].astype(f32)
        count, summed = pending.get((dz, dx), (0, 0.0))
        pending[dz, dx] = (count + 1, summed + value)
        if count + 1 == n_y:
            named = jnp.where(routes_ref[...] == expert, route_weights_ref[...], 0.0)
            weight = to_column(jnp.sum(named, axis=0, keepdims=True))
            total += weight * pending[dz, dx][1].astype(bf16).astype(f32)
    out_ref[...] = total.astype(bf16)

    if tp_peers:
        pltpu.make_async_copy(part_in_ref, part_in_ref, sent_sems.at[0]).wait()
    if remote:
        pltpu.make_async_copy(back_in_ref, back_in_ref, sent_sems.at[1]).wait()
        pltpu.make_async_copy(back_in_ref, back_in_ref, sent_sems.at[4]).wait()
    if n_core > 1:
        pltpu.make_async_copy(piece_in_ref, piece_in_ref, sent_sems.at[2]).wait()
        pltpu.make_async_copy(piece_in_ref, piece_in_ref, sent_sems.at[3]).wait()


def per_device(
    tokens,
    lengths,
    key_cache,
    value_cache,
    attn_gain,
    w_query,
    w_key,
    w_value,
    mix_lambda,
    head_gain,
    w_out,
    ffn_gain,
    w_gate,
    w_up,
    w_down,
    routes,
    route_weights,
):
    n_ep, n_tp = lax.axis_size("ep"), lax.axis_size("tp")
    seq_dev, model_width = tokens.shape
    cache_len, group_heads, head_width = key_cache.shape[1:]
    flat_len = cache_len * group_heads
    group_rows = group_heads * seq_dev
    block = model_width // n_tp
    n_y = n_tp // 2 if n_tp % 2 == 0 else n_tp
    n_x = 2 ** ((n_ep.bit_length() - 1) // 2)
    n_x = n_x if n_ep % n_x == 0 else 1
    others = max(n_ep * n_y - 1, 1)
    operands = (
        lengths.reshape(1, seq_dev),
        mix_lambda.reshape(1, group_heads),
        tokens,
        attn_gain.reshape(1, model_width),
        head_gain.reshape(1, head_width),
        ffn_gain.reshape(1, model_width),
        routes.T,
        route_weights.T,
        w_query.reshape(model_width * group_heads, head_width),
        w_key.reshape(model_width * group_heads, head_width),
        w_value.reshape(model_width * group_heads, head_width),
        key_cache.reshape(seq_dev, flat_len, head_width),
        value_cache.reshape(seq_dev, flat_len, head_width),
        w_out.reshape(group_heads * head_width, model_width),
        w_gate[0],
        w_up[0],
        w_down[0],
    )
    vmem = pltpu.VMEM
    return pl.pallas_call(
        functools.partial(layer_kernel, n_ep, n_tp, n_x, group_heads),
        out_shape=jax.ShapeDtypeStruct((seq_dev, block), bf16),
        in_specs=[pl.BlockSpec(memory_space=pltpu.HBM)] * len(operands),
        out_specs=pl.BlockSpec(memory_space=vmem),
        scratch_shapes=[vmem(operand.shape, operand.dtype) for operand in operands]
        + [
            vmem((2 * group_rows, seq_dev * head_width), bf16),
            vmem((2 * group_rows, flat_len), f32),
            vmem((group_rows, flat_len), bf16),
            vmem((n_tp, seq_dev, block), bf16),
            vmem((max(n_tp - 1, 1), seq_dev, block), bf16),
            vmem((n_ep * seq_dev, model_width), bf16),
            vmem((n_ep * seq_dev, model_width), bf16),
            vmem((n_y, n_ep, seq_dev, block), bf16),
            vmem((n_y, n_ep, seq_dev, block), bf16),
            vmem((n_y, n_ep, seq_dev, block), bf16),
            vmem((others, seq_dev, block), bf16),
            pltpu.SemaphoreType.DMA((15,)),
            pltpu.SemaphoreType.DMA((key_chunks,)),
            pltpu.SemaphoreType.DMA((seq_dev // 2,)),
            pltpu.SemaphoreType.DMA((1,)),
            pltpu.SemaphoreType.DMA((n_ep * n_y,)),
            pltpu.SemaphoreType.DMA((1,)),
            pltpu.SemaphoreType.DMA((n_y,)),
            pltpu.SemaphoreType.DMA((n_ep * n_y,)),
            pltpu.SemaphoreType.DMA((5,)),
        ],
        compiler_params=pltpu.CompilerParams(
            collective_id=0, has_side_effects=True, vmem_limit_bytes=58 * 2**20
        ),
    )(*operands)


def solution(mesh):
    placed = (
        P("ep", None),
        P("ep"),
        P("ep", None, "tp", None),
        P("ep", None, "tp", None),
        P(),
        P(None, "tp", None),
        P(None, "tp", None),
        P(None, "tp", None),
        P("tp"),
        P(),
        P("tp", None, None),
        P(),
        P("ep", None, "tp"),
        P("ep", None, "tp"),
        P("ep", "tp", None),
        P("ep", None),
        P("ep", None),
    )
    return jax.shard_map(
        per_device, mesh=mesh, in_specs=placed, out_specs=P("ep", "tp"), check_vma=False
    )
```

```python
import functools

import jax
import jax.numpy as jnp
from jax import lax
from jax.experimental import pallas as pl
from jax.experimental.pallas import tpu as pltpu
from jax.sharding import PartitionSpec as P

epsilon = 1e-06
clamp_limit = 7.0
sigmoid_slope = 1.702
branch_scale = 0.2
MESH = pl.DeviceIdType.MESH
f32, bf16 = jnp.float32, jnp.bfloat16
lane_tile = 128
wide_tile = 256
key_chunks = 4
lent_early = 2
barrier_chunk = 2
value_chunks = 4


def norm_rows(wide, gain):
    return wide * lax.rsqrt(jnp.mean(wide * wide, axis=-1, keepdims=True) + epsilon) * gain


def dot(left, right):
    return jnp.dot(left, right, preferred_element_type=f32)


def dot_rows(left, right):
    return lax.dot_general(left, right, (((1,), (1,)), ((), ())), preferred_element_type=f32)


def iota(shape, axis):
    return lax.broadcasted_iota(jnp.int32, shape, axis)


def to_column(row):
    size = row.shape[1]
    eye = iota((size, size), 0) == iota((size, size), 1)
    return jnp.sum(jnp.where(eye, row, jnp.zeros_like(row)), axis=1, keepdims=True)


def layer_kernel(
    n_ep,
    n_tp,
    n_x,
    group_heads,
    lengths_hbm,
    lambda_hbm,
    tokens_hbm,
    attn_gain_hbm,
    head_gain_hbm,
    ffn_gain_hbm,
    routes_hbm,
    route_weights_hbm,
    w_query_hbm,
    w_key_hbm,
    w_value_hbm,
    key_hbm,
    value_hbm,
    w_out_hbm,
    w_gate_hbm,
    w_up_hbm,
    w_down_hbm,
    out_ref,
    lengths_ref,
    lambda_ref,
    tokens_ref,
    attn_gain_ref,
    head_gain_ref,
    ffn_gain_ref,
    routes_ref,
    route_weights_ref,
    w_query_ref,
    w_key_ref,
    w_value_ref,
    key_ref,
    value_ref,
    w_out_ref,
    w_gate_ref,
    w_up_ref,
    w_down_ref,
    query_ref,
    score_ref,
    mix_ref,
    part_ref,
    part_in_ref,
    residual_ref,
    rows_ref,
    back_ref,
    back_in_ref,
    load_sems,
    key_sems,
    value_sems,
    lent_sems,
    part_sems,
    rows_sems,
    back_sems,
    sent_sems,
):
    my_ep, my_tp = lax.axis_index("ep"), lax.axis_index("tp")
    n_core = 2 if n_tp % 2 == 0 and n_ep % 2 == 0 else 1
    n_y = n_tp // n_core
    n_z = n_ep // n_x
    my_y, my_core = my_tp // n_core, lax.rem(my_tp, n_core)
    my_z, my_x = my_ep // n_x, lax.rem(my_ep, n_x)
    seq_dev, model_width = tokens_ref.shape
    flat_len, head_width = key_ref.shape[1:]
    half_width = head_width // 2
    block = out_ref.shape[1]

    singles = (
        (tokens_hbm, tokens_ref),
        (attn_gain_hbm, attn_gain_ref),
        (w_query_hbm, w_query_ref),
        (w_key_hbm, w_key_ref),
        (w_value_hbm, w_value_ref),
        (lengths_hbm, lengths_ref),
        (lambda_hbm, lambda_ref),
        (head_gain_hbm, head_gain_ref),
        (ffn_gain_hbm, ffn_gain_ref),
        (routes_hbm, routes_ref),
        (route_weights_hbm, route_weights_ref),
        (w_out_hbm, w_out_ref),
        (w_gate_hbm, w_gate_ref.at[0]),
        (w_up_hbm, w_up_ref.at[0]),
        (w_down_hbm, w_down_ref.at[0]),
    )
    loads = [
        pltpu.make_async_copy(source, target, load_sems.at[i])
        for i, (source, target) in enumerate(singles)
    ]
    chunk = flat_len // key_chunks
    key_loads = [
        pltpu.make_async_copy(
            key_hbm.at[:, pl.ds(j * chunk, chunk), :],
            key_ref.at[:, pl.ds(j * chunk, chunk), :],
            key_sems.at[j],
        )
        for j in range(key_chunks)
    ]
    value_group = seq_dev // value_chunks
    value_loads = [
        pltpu.make_async_copy(
            value_hbm.at[pl.ds(i * value_group, value_group)],
            value_ref.at[pl.ds(i * value_group, value_group)],
            value_sems.at[i],
        )
        for i in range(value_chunks)
    ]
    for copy in loads[:11]:
        copy.start()
    for copy in key_loads:
        copy.start(priority=1)

    def device(dz, dx, dy, core):
        ep = lax.rem(my_z + dz, n_z) * n_x + lax.rem(my_x + dx, n_x)
        return ep, lax.rem(my_y + dy, n_y) * n_core + core

    def hops(offset):
        dz, dx = offset
        return min(dz, n_z - dz) + min(dx, n_x - dx)

    slots = sorted([(dz, dx) for dz in range(n_z) for dx in range(n_x)], key=hops)
    held = n_ep // n_core
    far_y = sorted(range(n_y), key=lambda dy: -min(dy, n_y - dy))
    far_first = [(i, dy) for i in range(n_ep)[::-1] for dy in far_y]
    tp_peers = [(dy, dc) for dy in range(n_y) for dc in range(n_core)][1:]
    sibling_core = lax.rem(my_core + 1, n_core)

    def my_offset(j):
        dz, dx = slots[j]
        for core in range(1, n_core):
            next_z, next_x = slots[j + core * held]
            last_z, last_x = slots[j + (core - 1) * held]
            past = (my_core + n_core - core) // n_core
            dz, dx = dz + (next_z - last_z) * past, dx + (next_x - last_x) * past
        return dz, dx

    barrier = pltpu.get_barrier_semaphore()
    def greet(peer):
        pl.semaphore_signal(barrier, inc=1, device_id=peer, device_id_type=MESH)

    for i, dy in far_first[:-1]:
        for core in range(n_core):
            greet(device(*slots[i], dy, core))
    for dc in range(1, n_core):
        greet(device(0, 0, 0, lax.rem(my_core + dc, n_core)))
    greeted = n_ep * n_tp - 1

    loads[0].wait()
    loads[1].wait()
    for copy in value_loads:
        copy.start(priority=1)
    normed = norm_rows(tokens_ref[...].astype(f32), attn_gain_ref[...]).astype(bf16)
    span = wide_tile * group_heads
    blocks = model_width // wide_tile
    stacked = jnp.concatenate(
        [normed[:, b * wide_tile : (b + 1) * wide_tile] for b in range(blocks)], axis=0
    )
    if group_heads > 1:
        spread = iota((wide_tile, span), 1) // group_heads == iota((wide_tile, span), 0)
        stacked = dot(stacked, spread.astype(f32).astype(bf16))
    else:
        stacked = stacked.astype(f32)
    lane_head = lax.rem(iota((1, span), 1), group_heads)
    left = jnp.concatenate(
        [
            jnp.concatenate(
                [
                    jnp.where(
                        lane_head == h, stacked[b * seq_dev : (b + 1) * seq_dev], 0.0
                    ).astype(bf16)
                    for h in range(group_heads)
                ],
                axis=0,
            )
            for b in range(blocks)
        ],
        axis=1,
    )
    loads[2].wait()
    queries = dot(left, w_query_ref[...]).astype(bf16).astype(f32)
    loads[3].wait()
    key_new = dot(left, w_key_ref[...]).astype(bf16).astype(f32)
    loads[4].wait()
    value_new = dot(left, w_value_ref[...]).astype(bf16).astype(f32)

    score_scale = half_width ** (-0.5)
    group_rows = group_heads * seq_dev
    first_half = iota((1, head_width), 1) < half_width
    halves = jnp.concatenate(
        [jnp.where(first_half, queries, 0.0), jnp.where(first_half, 0.0, queries)], axis=0
    )
    own = jnp.sum(halves * jnp.concatenate([key_new, key_new], axis=0), axis=-1, keepdims=True)
    own = own * score_scale
    row_seq = lax.rem(iota((2 * group_rows, 1), 0), seq_dev)
    row_head = lax.rem(iota((2 * group_rows, 1), 0) // seq_dev, group_heads)
    for s in range(seq_dev):
        query_ref[:, s * head_width : (s + 1) * head_width] = jnp.where(
            row_seq == s, halves, 0.0
        ).astype(bf16)

    for load in loads[5:11]:
        load.wait()
    limit = to_column(lengths_ref[...]) * group_heads
    limit = jnp.concatenate([limit] * (2 * group_heads), axis=0)
    balance = jnp.concatenate(
        [jnp.broadcast_to(lambda_ref[0:1, h : h + 1], (seq_dev, 1)) for h in range(group_heads)],
        axis=0,
    )

    def masked(j):
        columns = slice(j * chunk, (j + 1) * chunk)
        column = iota((1, chunk), 1) + j * chunk
        live = (column < limit) & (lax.rem(column, group_heads) == row_head)
        scores = jnp.where(live, score_ref[:, columns] * score_scale, -jnp.inf)
        score_ref[:, columns] = scores
        return jnp.max(scores, axis=-1, keepdims=True)

    depth = w_up_hbm.shape[0] // 2
    lent = [
        pltpu.make_async_remote_copy(
            src_ref=source,
            dst_ref=target,
            send_sem=lent_sems.at[0, i],
            recv_sem=lent_sems.at[1, i],
            device_id=device(0, 0, 0, sibling_core),
            device_id_type=MESH,
        )
        for i, (source, target) in enumerate(
            (
                (w_gate_hbm, w_gate_ref.at[n_core - 1]),
                (w_up_hbm.at[pl.ds(0, depth)], w_up_ref.at[n_core - 1, pl.ds(0, depth)]),
                (w_up_hbm.at[pl.ds(depth, depth)], w_up_ref.at[n_core - 1, pl.ds(depth, depth)]),
                (w_down_hbm, w_down_ref.at[n_core - 1]),
            )
        )
    ]
    lent = lent if n_core > 1 else []
    peak = own
    for j in range(key_chunks):
        if j == barrier_chunk:
            pl.semaphore_wait(barrier, greeted)
            for copy in lent[:lent_early]:
                copy.start()
        key_loads[j].wait()
        if j == key_chunks - 1:
            loads[11].start(priority=1)
        keys = jnp.concatenate(
            [key_ref[s, j * chunk : (j + 1) * chunk, :] for s in range(seq_dev)], axis=1
        )
        score_ref[:, j * chunk : (j + 1) * chunk] = dot_rows(query_ref[...], keys)
        if j:
            peak = jnp.maximum(peak, masked(j - 1))
    peak = jnp.maximum(peak, masked(key_chunks - 1))
    own_weight = jnp.exp(own - peak)
    denominator = own_weight
    for j in range(key_chunks):
        weights = jnp.exp(score_ref[:, j * chunk : (j + 1) * chunk] - peak)
        score_ref[:, j * chunk : (j + 1) * chunk] = weights
        denominator = denominator + jnp.sum(weights, axis=-1, keepdims=True)
    inverse = 1.0 / denominator
    own_share = own_weight * inverse
    own_mix = own_share[:group_rows] - balance * own_share[group_rows:]
    own_mix = own_mix.astype(bf16).astype(f32)
    minuend, subtrahend = inverse[:group_rows], balance * inverse[group_rows:]
    for j in range(key_chunks):
        columns = slice(j * chunk, (j + 1) * chunk)
        mix_ref[:, columns] = (
            score_ref[:group_rows, columns] * minuend - score_ref[group_rows:, columns] * subtrahend
        ).astype(bf16)

    heads_out = own_mix * value_new
    group_seq = row_seq[:group_rows]
    for i in range(value_chunks):
        value_loads[i].wait()
        if i == 0:
            for copy in loads[12:]:
                copy.start(priority=1)
        members = range(i * value_group, (i + 1) * value_group)
        values = jnp.concatenate([value_ref[s] for s in members], axis=1)
        mixed = dot(mix_ref[...], values)
        for k, s in enumerate(members):
            heads_out = heads_out + jnp.where(
                group_seq == s, mixed[:, k * head_width : (k + 1) * head_width], 0.0
            )
    heads = norm_rows(heads_out, head_gain_ref[...] * branch_scale).astype(bf16)
    heads = jnp.concatenate(
        [heads[h * seq_dev : (h + 1) * seq_dev] for h in range(group_heads)], axis=1
    )

    loads[11].wait()
    for t in range(n_tp):
        part_ref[t] = dot(heads, w_out_ref[:, t * block : (t + 1) * block]).astype(bf16)

    def column_block(tp):
        return pl.ds(pl.multiple_of(tp * block, block), block)

    def row_block(slot):
        return slice(slot * seq_dev, (slot + 1) * seq_dev)

    for i, (dy, dc) in enumerate(tp_peers):
        peer = device(0, 0, dy, lax.rem(my_core + dc, n_core))
        pltpu.make_async_remote_copy(
            src_ref=part_ref.at[peer[1]],
            dst_ref=part_in_ref.at[i],
            send_sem=sent_sems.at[0],
            recv_sem=part_sems.at[0],
            device_id=peer,
            device_id_type=MESH,
        ).start()
    own_columns = column_block(my_tp)
    attention = part_ref[my_tp].astype(f32)
    if tp_peers:
        pltpu.make_async_copy(part_in_ref, part_in_ref, part_sems.at[0]).wait()
        for i in range(len(tp_peers)):
            attention += part_in_ref[i].astype(f32)
    residual_ref[...] = (tokens_ref[:, own_columns].astype(f32) + attention).astype(bf16)

    def rows_copy(j, tp, peer, recv):
        return pltpu.make_async_remote_copy(
            src_ref=residual_ref,
            dst_ref=rows_ref.at[row_block(j), column_block(tp)],
            send_sem=sent_sems.at[1],
            recv_sem=recv,
            device_id=peer,
            device_id_type=MESH,
        )

    is_home = my_core == 0
    for i, dy in far_first:
        core, j = i // held, i % held
        copy = rows_copy(j, my_tp, device(*slots[i], dy, core), rows_sems.at[j, dy, my_core])
        if (i, dy) == (0, 0):
            pl.when(jnp.logical_not(is_home))(copy.start)
        else:
            copy.start()

    for copy in lent[lent_early:]:
        copy.start()

    @pl.when(is_home)
    def _():
        rows_ref[row_block(0), own_columns] = residual_ref[...]

    for j in range(held):
        for dy in range(n_y):
            for core in range(n_core):
                tp = device(0, 0, n_y - dy, core)[1]
                copy = rows_copy(j, tp, (my_ep, my_tp), rows_sems.at[j, dy, core])
                if (j, dy, core) == (0, 0, 0):
                    pl.when(jnp.logical_not(is_home))(copy.wait_recv)
                else:
                    copy.wait_recv()

    for load in loads[12:]:
        load.wait()
    for copy in lent:
        copy.wait_recv()
    normed = norm_rows(rows_ref[...].astype(f32), ffn_gain_ref[...]).astype(bf16)
    activated = []
    for k in range(n_core):
        gate_value = jnp.minimum(dot(normed, w_gate_ref[k]), clamp_limit)
        up_value = jnp.clip(dot(normed, w_up_ref[k]), -clamp_limit, clamp_limit)
        activated.append(
            (
                (up_value + 1.0) * gate_value * jax.nn.sigmoid(sigmoid_slope * gate_value)
            ).astype(bf16)
        )
    for dy in far_y:
        for core in range(n_core):
            columns = column_block(device(0, 0, dy, core)[1])
            share = sum(dot(activated[k], w_down_ref[k, :, columns]) for k in range(n_core))
            back_ref[dy, core] = share.astype(bf16).reshape(held, seq_dev, block)
        for j in range(held)[::-1]:
            dz, dx = my_offset(j)
            place = j + held * my_core
            for core in range(n_core):
                copy = pltpu.make_async_remote_copy(
                    src_ref=back_ref.at[dy, core, j],
                    dst_ref=back_in_ref.at[dy, place],
                    send_sem=sent_sems.at[2],
                    recv_sem=back_sems.at[place, dy],
                    device_id=device(n_z - dz, n_x - dx, dy, core),
                    device_id_type=MESH,
                )
                if (j, dy, core) == (0, 0, 0):
                    pl.when(jnp.logical_not(is_home))(copy.start)
                else:
                    copy.start()

    @pl.when(is_home)
    def _():
        back_in_ref[0, 0] = back_ref[0, 0, 0]

    total = residual_ref[...].astype(f32)
    for i in range(n_ep):
        summed = 0.0
        for dy in far_y:
            arrived = back_in_ref.at[dy, i]
            copy = pltpu.make_async_copy(arrived, arrived, back_sems.at[i, dy])
            if (i, dy) == (0, 0):
                pl.when(jnp.logical_not(is_home))(copy.wait)
            else:
                copy.wait()
            summed = summed + back_in_ref[dy, i].astype(f32)
        named = jnp.where(routes_ref[...] == device(*slots[i], 0, 0)[0], route_weights_ref[...], 0.0)
        weight = to_column(jnp.sum(named, axis=0, keepdims=True))
        total += weight * summed.astype(bf16).astype(f32)
    out_ref[...] = total.astype(bf16)

    if tp_peers:
        pltpu.make_async_copy(part_in_ref, part_in_ref, sent_sems.at[0]).wait()
    for copy in lent:
        copy.wait_send()
    every = back_in_ref.at[pl.ds(0, n_y)]
    fewer = back_in_ref.at[0, pl.ds(0, n_ep - 1)]
    rest = back_in_ref.at[pl.ds(1, n_y - 1)] if n_y > 1 else None
    for sem in (sent_sems.at[1], sent_sems.at[2]):

        @pl.when(is_home)
        def _():
            pltpu.make_async_copy(fewer, fewer, sem).wait()
            if n_y > 1:
                pltpu.make_async_copy(rest, rest, sem).wait()

        @pl.when(jnp.logical_not(is_home))
        def _():
            pltpu.make_async_copy(every, every, sem).wait()


def per_device(
    tokens,
    lengths,
    key_cache,
    value_cache,
    attn_gain,
    w_query,
    w_key,
    w_value,
    mix_lambda,
    head_gain,
    w_out,
    ffn_gain,
    w_gate,
    w_up,
    w_down,
    routes,
    route_weights,
):
    n_ep, n_tp = lax.axis_size("ep"), lax.axis_size("tp")
    seq_dev, model_width = tokens.shape
    cache_len, group_heads, head_width = key_cache.shape[1:]
    flat_len = cache_len * group_heads
    group_rows = group_heads * seq_dev
    block = model_width // n_tp
    n_core = 2 if n_tp % 2 == 0 and n_ep % 2 == 0 else 1
    n_y = n_tp // n_core
    n_x = 2 ** ((n_ep.bit_length() - 1) // 2)
    n_x = n_x if n_ep % n_x == 0 else 1
    operands = (
        lengths.reshape(1, seq_dev),
        mix_lambda.reshape(1, group_heads),
        tokens,
        attn_gain.reshape(1, model_width),
        head_gain.reshape(1, head_width),
        ffn_gain.reshape(1, model_width),
        routes.T,
        route_weights.T,
        w_query.reshape(model_width * group_heads, head_width),
        w_key.reshape(model_width * group_heads, head_width),
        w_value.reshape(model_width * group_heads, head_width),
        key_cache.reshape(seq_dev, flat_len, head_width),
        value_cache.reshape(seq_dev, flat_len, head_width),
        w_out.reshape(group_heads * head_width, model_width),
        w_gate[0],
        w_up[0],
        w_down[0],
    )
    vmem = pltpu.VMEM
    return pl.pallas_call(
        functools.partial(layer_kernel, n_ep, n_tp, n_x, group_heads),
        out_shape=pltpu.VMEM((seq_dev, block), bf16),
        in_specs=[pl.BlockSpec(memory_space=pltpu.HBM)] * len(operands),
        out_specs=pl.BlockSpec(memory_space=vmem),
        scratch_shapes=[vmem(operand.shape, operand.dtype) for operand in operands[:-3]]
        + [vmem((n_core, *operand.shape), operand.dtype) for operand in operands[-3:]]
        + [
            vmem((2 * group_rows, seq_dev * head_width), bf16),
            vmem((2 * group_rows, flat_len), f32),
            vmem((group_rows, flat_len), bf16),
            vmem((n_tp, seq_dev, block), bf16),
            vmem((max(n_tp - 1, 1), seq_dev, block), bf16),
            vmem((seq_dev, block), bf16),
            vmem((n_ep // n_core * seq_dev, model_width), bf16),
            vmem((n_y, n_core, n_ep // n_core, seq_dev, block), bf16),
            vmem((n_y, n_ep, seq_dev, block), bf16),
            pltpu.SemaphoreType.DMA((15,)),
            pltpu.SemaphoreType.DMA((key_chunks,)),
            pltpu.SemaphoreType.DMA((value_chunks,)),
            pltpu.SemaphoreType.DMA((2, 4)),
            pltpu.SemaphoreType.DMA((1,)),
            pltpu.SemaphoreType.DMA((n_ep // n_core, n_y, n_core)),
            pltpu.SemaphoreType.DMA((n_ep, n_y)),
            pltpu.SemaphoreType.DMA((3,)),
        ],
        compiler_params=pltpu.CompilerParams(
            collective_id=0, has_side_effects=True, vmem_limit_bytes=58 * 2**20
        ),
    )(*operands)


def solution(mesh):
    placed = (
        P("ep", None),
        P("ep"),
        P("ep", None, "tp", None),
        P("ep", None, "tp", None),
        P(),
        P(None, "tp", None),
        P(None, "tp", None),
        P(None, "tp", None),
        P("tp"),
        P(),
        P("tp", None, None),
        P(),
        P("ep", None, "tp"),
        P("ep", None, "tp"),
        P("ep", "tp", None),
        P("ep", None),
        P("ep", None),
    )
    return jax.shard_map(
        per_device, mesh=mesh, in_specs=placed, out_specs=P("ep", "tp"), check_vma=False
    )
```

```python
import functools

import jax
import jax.numpy as jnp
from jax import lax
from jax.experimental import pallas as pl
from jax.experimental.pallas import tpu as pltpu
from jax.sharding import PartitionSpec as P

epsilon = 1e-06
clamp_limit = 7.0
sigmoid_slope = 1.702
branch_scale = 0.2
MESH = pl.DeviceIdType.MESH
f32, bf16 = jnp.float32, jnp.bfloat16
lane_tile = 128
wide_tile = 256
waves = 2
key_chunks = 2
value_chunks = 2


def norm_rows(wide, gain):
    return wide * lax.rsqrt(jnp.mean(wide * wide, axis=-1, keepdims=True) + epsilon) * gain


def dot(left, right):
    return jnp.dot(left, right, preferred_element_type=f32)


def dot_rows(left, right):
    return lax.dot_general(left, right, (((1,), (1,)), ((), ())), preferred_element_type=f32)


def iota(shape, axis):
    return lax.broadcasted_iota(jnp.int32, shape, axis)


def to_column(row):
    size = row.shape[1]
    eye = iota((size, size), 0) == iota((size, size), 1)
    return jnp.sum(jnp.where(eye, row, jnp.zeros_like(row)), axis=1, keepdims=True)


def layer_kernel(
    n_ep,
    n_tp,
    n_x,
    group_heads,
    lengths_hbm,
    lambda_hbm,
    tokens_hbm,
    attn_gain_hbm,
    head_gain_hbm,
    ffn_gain_hbm,
    routes_hbm,
    route_weights_hbm,
    w_query_hbm,
    w_key_hbm,
    w_value_hbm,
    key_hbm,
    value_hbm,
    w_out_hbm,
    w_gate_hbm,
    w_up_hbm,
    w_down_hbm,
    out_ref,
    lengths_ref,
    lambda_ref,
    tokens_ref,
    attn_gain_ref,
    head_gain_ref,
    ffn_gain_ref,
    routes_ref,
    route_weights_ref,
    w_query_ref,
    w_key_ref,
    w_value_ref,
    key_ref,
    value_ref,
    w_out_ref,
    w_gate_ref,
    w_up_ref,
    w_down_ref,
    query_ref,
    score_ref,
    mix_ref,
    part_ref,
    part_in_ref,
    residual_ref,
    rows_ref,
    hidden_ref,
    back_ref,
    back_in_ref,
    load_sems,
    key_sems,
    value_sems,
    lent_sems,
    part_sems,
    rows_sems,
    back_sems,
    sent_sems,
):
    my_ep, my_tp = lax.axis_index("ep"), lax.axis_index("tp")
    n_core = 2 if n_tp % 2 == 0 and n_ep % 2 == 0 else 1
    n_y = n_tp // n_core
    n_z = n_ep // n_x
    my_y, my_core = my_tp // n_core, lax.rem(my_tp, n_core)
    my_z, my_x = my_ep // n_x, lax.rem(my_ep, n_x)
    seq_dev, model_width = tokens_ref.shape
    flat_len, head_width = key_ref.shape[1:]
    half_width = head_width // 2
    block = out_ref.shape[1]

    singles = (
        (tokens_hbm, tokens_ref),
        (attn_gain_hbm, attn_gain_ref),
        (w_query_hbm, w_query_ref),
        (w_key_hbm, w_key_ref),
        (w_value_hbm, w_value_ref),
        (lengths_hbm, lengths_ref),
        (lambda_hbm, lambda_ref),
        (head_gain_hbm, head_gain_ref),
        (ffn_gain_hbm, ffn_gain_ref),
        (routes_hbm, routes_ref),
        (route_weights_hbm, route_weights_ref),
        (w_out_hbm, w_out_ref),
        (w_gate_hbm, w_gate_ref.at[0]),
        (w_up_hbm, w_up_ref.at[0]),
        (w_down_hbm, w_down_ref.at[0]),
    )
    loads = [
        pltpu.make_async_copy(source, target, load_sems.at[i])
        for i, (source, target) in enumerate(singles)
    ]
    chunk = flat_len // key_chunks
    wave = seq_dev // waves
    value_group = wave // value_chunks
    key_loads = [
        [
            pltpu.make_async_copy(
                key_hbm.at[pl.ds(w * wave, wave), pl.ds(j * chunk, chunk), :],
                key_ref.at[pl.ds(w * wave, wave), pl.ds(j * chunk, chunk), :],
                key_sems.at[w, j],
            )
            for j in range(key_chunks)
        ]
        for w in range(waves)
    ]
    value_loads = [
        [
            pltpu.make_async_copy(
                value_hbm.at[pl.ds(w * wave + i * value_group, value_group)],
                value_ref.at[pl.ds(w * wave + i * value_group, value_group)],
                value_sems.at[w, i],
            )
            for i in range(value_chunks)
        ]
        for w in range(waves)
    ]

    def start_bulk(copies):
        for copy in copies:
            copy.start(priority=1)

    for copy in loads[:11]:
        copy.start()
    start_bulk(key_loads[0])

    def device(dz, dx, dy, core):
        ep = lax.rem(my_z + dz, n_z) * n_x + lax.rem(my_x + dx, n_x)
        return ep, lax.rem(my_y + dy, n_y) * n_core + core

    def hops(offset):
        dz, dx = offset
        return min(dz, n_z - dz) + min(dx, n_x - dx)

    slots = sorted([(dz, dx) for dz in range(n_z) for dx in range(n_x)], key=hops)
    held = n_ep // n_core
    far_y = sorted(range(n_y), key=lambda dy: -min(dy, n_y - dy))
    far_first = [(i, dy) for i in range(n_ep)[::-1] for dy in far_y]
    tp_peers = [(dy, dc) for dy in range(n_y) for dc in range(n_core)][1:]
    sibling_core = lax.rem(my_core + 1, n_core)

    def my_offset(j):
        dz, dx = slots[j]
        for core in range(1, n_core):
            next_z, next_x = slots[j + core * held]
            last_z, last_x = slots[j + (core - 1) * held]
            past = (my_core + n_core - core) // n_core
            dz, dx = dz + (next_z - last_z) * past, dx + (next_x - last_x) * past
        return dz, dx

    barrier = pltpu.get_barrier_semaphore()

    def greet(peer):
        pl.semaphore_signal(barrier, inc=1, device_id=peer, device_id_type=MESH)

    for i, dy in far_first[:-1]:
        for core in range(n_core):
            greet(device(*slots[i], dy, core))
    for dc in range(1, n_core):
        greet(device(0, 0, 0, lax.rem(my_core + dc, n_core)))
    greeted = n_ep * n_tp - 1

    loads[0].wait()
    loads[1].wait()
    start_bulk(value_loads[0])
    normed = norm_rows(tokens_ref[...].astype(f32), attn_gain_ref[...]).astype(bf16)
    span = wide_tile * group_heads
    blocks = model_width // wide_tile
    stacked = jnp.concatenate(
        [normed[:, b * wide_tile : (b + 1) * wide_tile] for b in range(blocks)], axis=0
    )
    if group_heads > 1:
        spread = iota((wide_tile, span), 1) // group_heads == iota((wide_tile, span), 0)
        stacked = dot(stacked, spread.astype(f32).astype(bf16))
    else:
        stacked = stacked.astype(f32)
    lane_head = lax.rem(iota((1, span), 1), group_heads)
    left = jnp.concatenate(
        [
            jnp.concatenate(
                [
                    jnp.where(
                        lane_head == h, stacked[b * seq_dev : (b + 1) * seq_dev], 0.0
                    ).astype(bf16)
                    for h in range(group_heads)
                ],
                axis=0,
            )
            for b in range(blocks)
        ],
        axis=1,
    )
    loads[2].wait()
    queries = dot(left, w_query_ref[...]).astype(bf16).astype(f32)
    loads[3].wait()
    key_new = dot(left, w_key_ref[...]).astype(bf16).astype(f32)
    loads[4].wait()
    value_new = dot(left, w_value_ref[...]).astype(bf16).astype(f32)
    start_bulk(key_loads[1])

    score_scale = half_width ** (-0.5)
    first_half = iota((1, head_width), 1) < half_width
    halves = jnp.concatenate(
        [jnp.where(first_half, queries, 0.0), jnp.where(first_half, 0.0, queries)], axis=0
    )
    own = jnp.sum(halves * jnp.concatenate([key_new, key_new], axis=0), axis=-1, keepdims=True)
    own = own * score_scale
    for load in loads[5:11]:
        load.wait()
    limit = to_column(lengths_ref[...]) * group_heads
    limit = jnp.concatenate([limit] * (2 * group_heads), axis=0)
    balance = jnp.concatenate(
        [jnp.broadcast_to(lambda_ref[0:1, h : h + 1], (wave, 1)) for h in range(group_heads)],
        axis=0,
    )
    wave_rows = group_heads * wave
    row_seq = lax.rem(iota((2 * wave_rows, 1), 0), wave)
    row_head = lax.rem(iota((2 * wave_rows, 1), 0) // wave, group_heads)

    def of_wave(rows, w):
        first = range(w * wave, rows.shape[0], seq_dev)
        return jnp.concatenate([rows[r : r + wave] for r in first], axis=0)

    depth = w_down_hbm.shape[0] // 2
    parts = ((0, depth), (depth, depth))
    lent = [
        pltpu.make_async_remote_copy(
            src_ref=source,
            dst_ref=target,
            send_sem=lent_sems.at[0, i],
            recv_sem=lent_sems.at[1, i],
            device_id=device(0, 0, 0, sibling_core),
            device_id_type=MESH,
        )
        for i, (source, target) in enumerate(
            [(w_gate_hbm, w_gate_ref.at[n_core - 1]), (w_up_hbm, w_up_ref.at[n_core - 1])]
            + [
                (w_down_hbm.at[pl.ds(*part)], w_down_ref.at[n_core - 1, pl.ds(*part)])
                for part in parts
            ]
        )
    ]
    lent = lent if n_core > 1 else []

    def lend(i):
        for copy in lent[i : i + 1]:
            copy.start()

    def share_weights(w):
        limits = of_wave(limit, w)
        own_score = of_wave(own, w)
        wave_halves = of_wave(halves, w)
        for s in range(wave):
            query_ref[w, :, s * head_width : (s + 1) * head_width] = jnp.where(
                row_seq == s, wave_halves, 0.0
            ).astype(bf16)

        def masked(j):
            columns = slice(j * chunk, (j + 1) * chunk)
            column = iota((1, chunk), 1) + j * chunk
            live = (column < limits) & (lax.rem(column, group_heads) == row_head)
            scores = jnp.where(live, score_ref[w, :, columns] * score_scale, -jnp.inf)
            score_ref[w, :, columns] = scores
            return jnp.max(scores, axis=-1, keepdims=True)

        peak = own_score
        for j in range(key_chunks):
            key_loads[w][j].wait()
            if (w, j) == (0, 0):
                loads[11].start()
                start_bulk(value_loads[1])
            keys = jnp.concatenate(
                [
                    key_ref[w * wave + s, j * chunk : (j + 1) * chunk, :]
                    for s in range(wave)
                ],
                axis=1,
            )
            score_ref[w, :, j * chunk : (j + 1) * chunk] = dot_rows(query_ref[w], keys)
            if j:
                peak = jnp.maximum(peak, masked(j - 1))
        peak = jnp.maximum(peak, masked(key_chunks - 1))
        own_weight = jnp.exp(own_score - peak)
        denominator = own_weight
        for j in range(key_chunks):
            columns = slice(j * chunk, (j + 1) * chunk)
            weights = jnp.exp(score_ref[w, :, columns] - peak)
            score_ref[w, :, columns] = weights
            denominator = denominator + jnp.sum(weights, axis=-1, keepdims=True)
        inverse = 1.0 / denominator
        own_share = own_weight * inverse
        own_mix = own_share[:wave_rows] - balance * own_share[wave_rows:]
        minuend, subtrahend = inverse[:wave_rows], balance * inverse[wave_rows:]
        for j in range(key_chunks):
            columns = slice(j * chunk, (j + 1) * chunk)
            mix_ref[w, :, columns] = (
                score_ref[w, :wave_rows, columns] * minuend
                - score_ref[w, wave_rows:, columns] * subtrahend
            ).astype(bf16)
        return own_mix.astype(bf16).astype(f32)

    def mix_values(w, own_mix, before_last):
        heads_out = own_mix * of_wave(value_new, w)
        for i in range(value_chunks):
            if i == value_chunks - 1:
                before_last()
            value_loads[w][i].wait()
            members = range(i * value_group, (i + 1) * value_group)
            values = jnp.concatenate([value_ref[w * wave + s] for s in members], axis=1)
            mixed = dot(mix_ref[w], values)
            for k, s in enumerate(members):
                heads_out = heads_out + jnp.where(
                    row_seq[:wave_rows] == s, mixed[:, k * head_width : (k + 1) * head_width], 0.0
                )
        return heads_out

    def column_block(tp):
        return pl.ds(pl.multiple_of(tp * block, block), block)

    is_home = my_core == 0
    own_columns = column_block(my_tp)

    def project(w, heads_out):
        heads = norm_rows(heads_out, head_gain_ref[...] * branch_scale)
        heads = jnp.concatenate(
            [heads[h * wave : (h + 1) * wave] for h in range(group_heads)], axis=1
        ).astype(bf16)
        for t in range(n_tp):
            part_ref[w, t] = dot(heads, w_out_ref[:, t * block : (t + 1) * block]).astype(bf16)
        for i, (dy, dc) in enumerate(tp_peers):
            peer = device(0, 0, dy, lax.rem(my_core + dc, n_core))
            pltpu.make_async_remote_copy(
                src_ref=part_ref.at[w, peer[1]],
                dst_ref=part_in_ref.at[w, i],
                send_sem=sent_sems.at[0],
                recv_sem=part_sems.at[w],
                device_id=peer,
                device_id_type=MESH,
            ).start()

    def rows_copy(w, j, tp, peer, recv):
        return pltpu.make_async_remote_copy(
            src_ref=residual_ref.at[w],
            dst_ref=rows_ref.at[w, j, tp],
            send_sem=sent_sems.at[1],
            recv_sem=recv,
            device_id=peer,
            device_id_type=MESH,
        )

    def spread_rows(w):
        attention = part_ref[w, my_tp].astype(f32)
        if tp_peers:
            landed = part_in_ref.at[w]
            pltpu.make_async_copy(landed, landed, part_sems.at[w]).wait()
            for i in range(len(tp_peers)):
                attention += part_in_ref[w, i].astype(f32)
        mine = tokens_ref[:, own_columns].astype(f32)[w * wave : (w + 1) * wave]
        residual_ref[w] = (mine + attention).astype(bf16)
        for i, dy in far_first:
            core, j = i // held, i % held
            peer = device(*slots[i], dy, core)
            copy = rows_copy(w, j, my_tp, peer, rows_sems.at[w, j, dy, my_core])
            if (i, dy) == (0, 0):
                pl.when(jnp.logical_not(is_home))(copy.start)
            else:
                copy.start()

        @pl.when(is_home)
        def _():
            rows_ref[w, 0, my_tp] = residual_ref[w]

    sources = [[(dy, core)] for core in range(n_core)[::-1] for dy in range(n_y)]

    def experts(w):
        squares = jnp.zeros((held * wave, 1), f32)
        for step, some in enumerate(sources):
            for dy, core in some:
                tp = device(0, 0, n_y - dy, core)[1]
                for j in range(held):
                    copy = rows_copy(w, j, tp, (my_ep, my_tp), rows_sems.at[w, j, dy, core])
                    if (j, dy, core) == (0, 0, 0):
                        pl.when(jnp.logical_not(is_home))(copy.wait_recv)
                    else:
                        copy.wait_recv()
            if (w, step) == (0, 0):
                for load in loads[12:14]:
                    load.wait()
                for copy in lent[:2]:
                    copy.wait_recv()
            scaled = []
            for dy, core in some:
                tp = device(0, 0, n_y - dy, core)[1]
                rows = jnp.concatenate(
                    [rows_ref[w, j, tp].astype(f32) for j in range(held)], axis=0
                )
                squares = squares + jnp.sum(rows * rows, axis=-1, keepdims=True)
                scaled.append((tp, (rows * ffn_gain_ref[:, column_block(tp)]).astype(bf16)))
            for k in range(n_core):
                for n, weight_ref in enumerate((w_gate_ref, w_up_ref)):
                    share = sum(dot(rows, weight_ref[k, column_block(tp), :]) for tp, rows in scaled)
                    if step:
                        share = share + hidden_ref[k, n]
                    hidden_ref[k, n] = share
        scale = lax.rsqrt(squares / model_width + epsilon)
        activated = []
        for k in range(n_core):
            gate_value = jnp.minimum(hidden_ref[k, 0] * scale, clamp_limit)
            up_value = jnp.clip(hidden_ref[k, 1] * scale, -clamp_limit, clamp_limit)
            activated.append(
                (
                    (up_value + 1.0) * gate_value * jax.nn.sigmoid(sigmoid_slope * gate_value)
                ).astype(bf16)
            )
        if w == 0:
            loads[14].wait()
            for copy in lent[2:]:
                copy.wait_recv()
        for dy in far_y:
            for core in range(n_core):
                columns = column_block(device(0, 0, dy, core)[1])
                share = sum(dot(activated[k], w_down_ref[k, :, columns]) for k in range(n_core))
                for j in range(held):
                    back_ref[w, dy, core, j] = share[j * wave : (j + 1) * wave].astype(bf16)
            for j in range(held)[::-1]:
                dz, dx = my_offset(j)
                place = j + held * my_core
                for core in range(n_core):
                    copy = pltpu.make_async_remote_copy(
                        src_ref=back_ref.at[w, dy, core, j],
                        dst_ref=back_in_ref.at[w, dy, place],
                        send_sem=sent_sems.at[2],
                        recv_sem=back_sems.at[w, place, dy],
                        device_id=device(n_z - dz, n_x - dx, dy, core),
                        device_id_type=MESH,
                    )
                    if (j, dy, core) == (0, 0, 0):
                        pl.when(jnp.logical_not(is_home))(copy.start)
                    else:
                        copy.start()

        @pl.when(is_home)
        def _():
            back_in_ref[w, 0, 0] = back_ref[w, 0, 0, 0]

    def collect(w, weights):
        total = residual_ref[w].astype(f32)
        for i in range(n_ep):
            summed = 0.0
            for dy in far_y:
                arrived = back_in_ref.at[w, dy, i]
                copy = pltpu.make_async_copy(arrived, arrived, back_sems.at[w, i, dy])
                if (i, dy) == (0, 0):
                    pl.when(jnp.logical_not(is_home))(copy.wait)
                else:
                    copy.wait()
                summed = summed + back_in_ref[w, dy, i].astype(f32)
            weight = weights[i][w * wave : (w + 1) * wave]
            total += weight * summed.astype(bf16).astype(f32)
        return total

    pl.semaphore_wait(barrier, greeted)
    lend(0)
    own_mix = share_weights(0)
    start_bulk(loads[12:])
    heads_out = mix_values(0, own_mix, lambda: None)
    loads[11].wait()
    project(0, heads_out)
    lend(1)
    own_mix = share_weights(1)
    heads_out = mix_values(1, own_mix, lambda: spread_rows(0))
    project(1, heads_out)
    lend(2)
    spread_rows(1)
    lend(3)
    weights = []
    for i in range(n_ep):
        named = jnp.where(routes_ref[...] == device(*slots[i], 0, 0)[0], route_weights_ref[...], 0.0)
        weights.append(to_column(jnp.sum(named, axis=0, keepdims=True)))
    experts(0)
    experts(1)
    total = jnp.concatenate([collect(w, weights) for w in range(waves)], axis=0)
    out_ref[...] = total.astype(bf16)

    if tp_peers:
        pltpu.make_async_copy(part_in_ref, part_in_ref, sent_sems.at[0]).wait()
    for copy in lent:
        copy.wait_send()
    for sem in (sent_sems.at[1], sent_sems.at[2]):
        for w in range(waves):
            fewer = back_in_ref.at[w, 0, pl.ds(0, n_ep - 1)]
            for dy in range(1, n_y):
                pltpu.make_async_copy(back_in_ref.at[w, dy], back_in_ref.at[w, dy], sem).wait()

            @pl.when(is_home)
            def _():
                pltpu.make_async_copy(fewer, fewer, sem).wait()

            @pl.when(jnp.logical_not(is_home))
            def _():
                pltpu.make_async_copy(back_in_ref.at[w, 0], back_in_ref.at[w, 0], sem).wait()


def per_device(
    tokens,
    lengths,
    key_cache,
    value_cache,
    attn_gain,
    w_query,
    w_key,
    w_value,
    mix_lambda,
    head_gain,
    w_out,
    ffn_gain,
    w_gate,
    w_up,
    w_down,
    routes,
    route_weights,
):
    n_ep, n_tp = lax.axis_size("ep"), lax.axis_size("tp")
    seq_dev, model_width = tokens.shape
    cache_len, group_heads, head_width = key_cache.shape[1:]
    flat_len = cache_len * group_heads
    wave = seq_dev // waves
    wave_rows = group_heads * wave
    block = model_width // n_tp
    n_core = 2 if n_tp % 2 == 0 and n_ep % 2 == 0 else 1
    n_y = n_tp // n_core
    n_x = 2 ** ((n_ep.bit_length() - 1) // 2)
    n_x = n_x if n_ep % n_x == 0 else 1
    operands = (
        lengths.reshape(1, seq_dev),
        mix_lambda.reshape(1, group_heads),
        tokens,
        attn_gain.reshape(1, model_width),
        head_gain.reshape(1, head_width),
        ffn_gain.reshape(1, model_width),
        routes.T,
        route_weights.T,
        w_query.reshape(model_width * group_heads, head_width),
        w_key.reshape(model_width * group_heads, head_width),
        w_value.reshape(model_width * group_heads, head_width),
        key_cache.reshape(seq_dev, flat_len, head_width),
        value_cache.reshape(seq_dev, flat_len, head_width),
        w_out.reshape(group_heads * head_width, model_width),
        w_gate[0],
        w_up[0],
        w_down[0],
    )
    vmem = pltpu.VMEM
    return pl.pallas_call(
        functools.partial(layer_kernel, n_ep, n_tp, n_x, group_heads),
        out_shape=pltpu.VMEM((seq_dev, block), bf16),
        in_specs=[pl.BlockSpec(memory_space=pltpu.HBM)] * len(operands),
        out_specs=pl.BlockSpec(memory_space=vmem),
        scratch_shapes=[vmem(operand.shape, operand.dtype) for operand in operands[:-3]]
        + [vmem((n_core, *operand.shape), operand.dtype) for operand in operands[-3:]]
        + [
            vmem((waves, 2 * wave_rows, wave * head_width), bf16),
            vmem((waves, 2 * wave_rows, flat_len), f32),
            vmem((waves, wave_rows, flat_len), bf16),
            vmem((waves, n_tp, wave, block), bf16),
            vmem((waves, max(n_tp - 1, 1), wave, block), bf16),
            vmem((waves, wave, block), bf16),
            vmem((waves, n_ep // n_core, n_tp, wave, block), bf16),
            vmem((n_core, 2, n_ep // n_core * wave, w_gate.shape[2]), f32),
            vmem((waves, n_y, n_core, n_ep // n_core, wave, block), bf16),
            vmem((waves, n_y, n_ep, wave, block), bf16),
            pltpu.SemaphoreType.DMA((15,)),
            pltpu.SemaphoreType.DMA((waves, key_chunks)),
            pltpu.SemaphoreType.DMA((waves, value_chunks)),
            pltpu.SemaphoreType.DMA((2, 4)),
            pltpu.SemaphoreType.DMA((waves,)),
            pltpu.SemaphoreType.DMA((waves, n_ep // n_core, n_y, n_core)),
            pltpu.SemaphoreType.DMA((waves, n_ep, n_y)),
            pltpu.SemaphoreType.DMA((3,)),
        ],
        compiler_params=pltpu.CompilerParams(
            collective_id=0, has_side_effects=True, vmem_limit_bytes=58 * 2**20
        ),
    )(*operands)


def solution(mesh):
    placed = (
        P("ep", None),
        P("ep"),
        P("ep", None, "tp", None),
        P("ep", None, "tp", None),
        P(),
        P(None, "tp", None),
        P(None, "tp", None),
        P(None, "tp", None),
        P("tp"),
        P(),
        P("tp", None, None),
        P(),
        P("ep", None, "tp"),
        P("ep", None, "tp"),
        P("ep", "tp", None),
        P("ep", None),
        P("ep", None),
    )
    return jax.shard_map(
        per_device, mesh=mesh, in_specs=placed, out_specs=P("ep", "tp"), check_vma=False
    )
```

```python
import functools

import jax
import jax.numpy as jnp
from jax import lax
from jax.experimental import pallas as pl
from jax.experimental.pallas import tpu as pltpu
from jax.sharding import PartitionSpec as P

epsilon = 1e-06
clamp_limit = 7.0
sigmoid_slope = 1.702
branch_scale = 0.2
MESH = pl.DeviceIdType.MESH
f32, bf16 = jnp.float32, jnp.bfloat16
lane_tile = 128
wide_tile = 256
waves = 2
enter_chunk = 1
lend_from = (0, 2, 4, 5, 6)
key_chunks = 2
value_chunks = 2


def norm_rows(wide, gain):
    return wide * lax.rsqrt(jnp.mean(wide * wide, axis=-1, keepdims=True) + epsilon) * gain


def dot(left, right):
    return jnp.dot(left, right, preferred_element_type=f32)


def dot_rows(left, right):
    return lax.dot_general(left, right, (((1,), (1,)), ((), ())), preferred_element_type=f32)


def iota(shape, axis):
    return lax.broadcasted_iota(jnp.int32, shape, axis)


def to_column(row):
    size = row.shape[1]
    eye = iota((size, size), 0) == iota((size, size), 1)
    return jnp.sum(jnp.where(eye, row, jnp.zeros_like(row)), axis=1, keepdims=True)


def layer_kernel(
    n_ep,
    n_tp,
    n_x,
    group_heads,
    lengths_hbm,
    lambda_hbm,
    tokens_hbm,
    attn_gain_hbm,
    head_gain_hbm,
    ffn_gain_hbm,
    routes_hbm,
    route_weights_hbm,
    w_query_hbm,
    w_key_hbm,
    w_value_hbm,
    key_hbm,
    value_hbm,
    w_out_hbm,
    w_gate_hbm,
    w_up_hbm,
    w_down_hbm,
    out_ref,
    lengths_ref,
    lambda_ref,
    tokens_ref,
    attn_gain_ref,
    head_gain_ref,
    ffn_gain_ref,
    routes_ref,
    route_weights_ref,
    w_query_ref,
    w_key_ref,
    w_value_ref,
    key_ref,
    value_ref,
    w_out_ref,
    w_gate_ref,
    w_up_ref,
    w_down_ref,
    query_ref,
    score_ref,
    mix_ref,
    part_ref,
    part_in_ref,
    residual_ref,
    rows_ref,
    hidden_ref,
    back_ref,
    back_in_ref,
    load_sems,
    key_sems,
    value_sems,
    lent_sems,
    part_sems,
    rows_sems,
    back_sems,
    sent_sems,
):
    my_ep, my_tp = lax.axis_index("ep"), lax.axis_index("tp")
    n_core = 2 if n_tp % 2 == 0 and n_ep % 2 == 0 else 1
    n_y = n_tp // n_core
    n_z = n_ep // n_x
    my_y, my_core = my_tp // n_core, lax.rem(my_tp, n_core)
    my_z, my_x = my_ep // n_x, lax.rem(my_ep, n_x)
    seq_dev, model_width = tokens_ref.shape
    flat_len, head_width = key_ref.shape[1:]
    half_width = head_width // 2
    block = out_ref.shape[1]

    singles = (
        (tokens_hbm, tokens_ref),
        (attn_gain_hbm, attn_gain_ref),
        (w_query_hbm, w_query_ref),
        (w_key_hbm, w_key_ref),
        (w_value_hbm, w_value_ref),
        (lengths_hbm, lengths_ref),
        (lambda_hbm, lambda_ref),
        (head_gain_hbm, head_gain_ref),
        (ffn_gain_hbm, ffn_gain_ref),
        (routes_hbm, routes_ref),
        (route_weights_hbm, route_weights_ref),
        (w_out_hbm, w_out_ref),
        (w_gate_hbm, w_gate_ref.at[0]),
        (w_up_hbm, w_up_ref.at[0]),
        (w_down_hbm, w_down_ref.at[0]),
    )
    loads = [
        pltpu.make_async_copy(source, target, load_sems.at[i])
        for i, (source, target) in enumerate(singles)
    ]
    chunk = flat_len // key_chunks
    wave = seq_dev // waves
    value_group = wave // value_chunks
    key_loads = [
        [
            pltpu.make_async_copy(
                key_hbm.at[pl.ds(w * wave, wave), pl.ds(j * chunk, chunk), :],
                key_ref.at[pl.ds(w * wave, wave), pl.ds(j * chunk, chunk), :],
                key_sems.at[w, j],
            )
            for j in range(key_chunks)
        ]
        for w in range(waves)
    ]
    value_loads = [
        [
            pltpu.make_async_copy(
                value_hbm.at[pl.ds(w * wave + i * value_group, value_group)],
                value_ref.at[pl.ds(w * wave + i * value_group, value_group)],
                value_sems.at[w, i],
            )
            for i in range(value_chunks)
        ]
        for w in range(waves)
    ]

    def start_bulk(copies):
        for copy in copies:
            copy.start(priority=1)

    for copy in loads[:11]:
        copy.start()
    start_bulk(key_loads[0])

    def device(dz, dx, dy, core):
        ep = lax.rem(my_z + dz, n_z) * n_x + lax.rem(my_x + dx, n_x)
        return ep, lax.rem(my_y + dy, n_y) * n_core + core

    def hops(offset):
        dz, dx = offset
        return min(dz, n_z - dz) + min(dx, n_x - dx)

    slots = sorted([(dz, dx) for dz in range(n_z) for dx in range(n_x)], key=hops)
    held = n_ep // n_core
    far_y = sorted(range(n_y), key=lambda dy: -min(dy, n_y - dy))
    far_first = [(i, dy) for i in range(n_ep)[::-1] for dy in far_y]
    tp_peers = [(dy, dc) for dy in range(n_y) for dc in range(n_core)][1:]
    sibling_core = lax.rem(my_core + 1, n_core)

    def my_offset(j):
        dz, dx = slots[j]
        for core in range(1, n_core):
            next_z, next_x = slots[j + core * held]
            last_z, last_x = slots[j + (core - 1) * held]
            past = (my_core + n_core - core) // n_core
            dz, dx = dz + (next_z - last_z) * past, dx + (next_x - last_x) * past
        return dz, dx

    barrier = pltpu.get_barrier_semaphore()

    def greet(peer):
        pl.semaphore_signal(barrier, inc=1, device_id=peer, device_id_type=MESH)

    for i, dy in far_first[:-1]:
        for core in range(n_core):
            greet(device(*slots[i], dy, core))
    for dc in range(1, n_core):
        greet(device(0, 0, 0, lax.rem(my_core + dc, n_core)))
    greeted = n_ep * n_tp - 1

    loads[0].wait()
    loads[1].wait()
    start_bulk(value_loads[0])
    normed = norm_rows(tokens_ref[...].astype(f32), attn_gain_ref[...]).astype(bf16)
    span = wide_tile * group_heads
    blocks = model_width // wide_tile
    stacked = jnp.concatenate(
        [normed[:, b * wide_tile : (b + 1) * wide_tile] for b in range(blocks)], axis=0
    )
    if group_heads > 1:
        spread = iota((wide_tile, span), 1) // group_heads == iota((wide_tile, span), 0)
        stacked = dot(stacked, spread.astype(f32).astype(bf16))
    else:
        stacked = stacked.astype(f32)
    lane_head = lax.rem(iota((1, span), 1), group_heads)
    left = jnp.concatenate(
        [
            jnp.concatenate(
                [
                    jnp.where(
                        lane_head == h, stacked[b * seq_dev : (b + 1) * seq_dev], 0.0
                    ).astype(bf16)
                    for h in range(group_heads)
                ],
                axis=0,
            )
            for b in range(blocks)
        ],
        axis=1,
    )
    loads[2].wait()
    queries = dot(left, w_query_ref[...]).astype(bf16).astype(f32)
    loads[3].wait()
    key_new = dot(left, w_key_ref[...]).astype(bf16).astype(f32)
    loads[4].wait()
    value_new = dot(left, w_value_ref[...]).astype(bf16).astype(f32)
    start_bulk(key_loads[1])

    score_scale = half_width ** (-0.5)
    first_half = iota((1, head_width), 1) < half_width
    halves = jnp.concatenate(
        [jnp.where(first_half, queries, 0.0), jnp.where(first_half, 0.0, queries)], axis=0
    )
    own = jnp.sum(halves * jnp.concatenate([key_new, key_new], axis=0), axis=-1, keepdims=True)
    own = own * score_scale
    for load in loads[5:11]:
        load.wait()
    limit = to_column(lengths_ref[...]) * group_heads
    limit = jnp.concatenate([limit] * (2 * group_heads), axis=0)
    balance = jnp.concatenate(
        [jnp.broadcast_to(lambda_ref[0:1, h : h + 1], (wave, 1)) for h in range(group_heads)],
        axis=0,
    )
    wave_rows = group_heads * wave
    row_seq = lax.rem(iota((2 * wave_rows, 1), 0), wave)
    row_head = lax.rem(iota((2 * wave_rows, 1), 0) // wave, group_heads)

    def of_wave(rows, w):
        first = range(w * wave, rows.shape[0], seq_dev)
        return jnp.concatenate([rows[r : r + wave] for r in first], axis=0)

    def pieces(source, target):
        depth = source.shape[0] // 2
        return [
            (source.at[pl.ds(first, depth)], target.at[n_core - 1, pl.ds(first, depth)])
            for first in (0, depth)
        ]

    lent = [
        pltpu.make_async_remote_copy(
            src_ref=source,
            dst_ref=target,
            send_sem=lent_sems.at[0, i],
            recv_sem=lent_sems.at[1, i],
            device_id=device(0, 0, 0, sibling_core),
            device_id_type=MESH,
        )
        for i, (source, target) in enumerate(
            pieces(w_gate_hbm, w_gate_ref)
            + pieces(w_up_hbm, w_up_ref)
            + pieces(w_down_hbm, w_down_ref)
        )
    ]
    lent = lent if n_core > 1 else []

    def lend(point):
        for copy in lent[lend_from[point] : lend_from[point + 1]]:
            copy.start()

    def enter():
        pl.semaphore_wait(barrier, greeted)
        lend(0)

    def share_weights(w):
        limits = of_wave(limit, w)
        own_score = of_wave(own, w)
        wave_halves = of_wave(halves, w)
        for s in range(wave):
            query_ref[w, :, s * head_width : (s + 1) * head_width] = jnp.where(
                row_seq == s, wave_halves, 0.0
            ).astype(bf16)

        def masked(j):
            columns = slice(j * chunk, (j + 1) * chunk)
            column = iota((1, chunk), 1) + j * chunk
            live = (column < limits) & (lax.rem(column, group_heads) == row_head)
            scores = jnp.where(live, score_ref[w, :, columns] * score_scale, -jnp.inf)
            score_ref[w, :, columns] = scores
            return jnp.max(scores, axis=-1, keepdims=True)

        peak = own_score
        for j in range(key_chunks):
            if (w, j) == (0, enter_chunk):
                enter()
            key_loads[w][j].wait()
            if (w, j) == (0, 0):
                loads[11].start()
                start_bulk(value_loads[1])
            keys = jnp.concatenate(
                [
                    key_ref[w * wave + s, j * chunk : (j + 1) * chunk, :]
                    for s in range(wave)
                ],
                axis=1,
            )
            score_ref[w, :, j * chunk : (j + 1) * chunk] = dot_rows(query_ref[w], keys)
            if j:
                peak = jnp.maximum(peak, masked(j - 1))
        peak = jnp.maximum(peak, masked(key_chunks - 1))
        own_weight = jnp.exp(own_score - peak)
        denominator = own_weight
        for j in range(key_chunks):
            columns = slice(j * chunk, (j + 1) * chunk)
            weights = jnp.exp(score_ref[w, :, columns] - peak)
            score_ref[w, :, columns] = weights
            denominator = denominator + jnp.sum(weights, axis=-1, keepdims=True)
        inverse = 1.0 / denominator
        own_share = own_weight * inverse
        own_mix = own_share[:wave_rows] - balance * own_share[wave_rows:]
        minuend, subtrahend = inverse[:wave_rows], balance * inverse[wave_rows:]
        for j in range(key_chunks):
            columns = slice(j * chunk, (j + 1) * chunk)
            mix_ref[w, :, columns] = (
                score_ref[w, :wave_rows, columns] * minuend
                - score_ref[w, wave_rows:, columns] * subtrahend
            ).astype(bf16)
        return own_mix.astype(bf16).astype(f32)

    def mix_values(w, own_mix, before_last):
        heads_out = own_mix * of_wave(value_new, w)
        for i in range(value_chunks):
            if i == value_chunks - 1:
                before_last()
            value_loads[w][i].wait()
            members = range(i * value_group, (i + 1) * value_group)
            values = jnp.concatenate([value_ref[w * wave + s] for s in members], axis=1)
            mixed = dot(mix_ref[w], values)
            for k, s in enumerate(members):
                heads_out = heads_out + jnp.where(
                    row_seq[:wave_rows] == s, mixed[:, k * head_width : (k + 1) * head_width], 0.0
                )
        return heads_out

    def column_block(tp):
        return pl.ds(pl.multiple_of(tp * block, block), block)

    is_home = my_core == 0
    own_columns = column_block(my_tp)

    def project(w, heads_out):
        heads = norm_rows(heads_out, head_gain_ref[...] * branch_scale)
        heads = jnp.concatenate(
            [heads[h * wave : (h + 1) * wave] for h in range(group_heads)], axis=1
        ).astype(bf16)
        for t in range(n_tp):
            part_ref[w, t] = dot(heads, w_out_ref[:, t * block : (t + 1) * block]).astype(bf16)
        for i, (dy, dc) in enumerate(tp_peers):
            peer = device(0, 0, dy, lax.rem(my_core + dc, n_core))
            pltpu.make_async_remote_copy(
                src_ref=part_ref.at[w, peer[1]],
                dst_ref=part_in_ref.at[w, i],
                send_sem=sent_sems.at[0],
                recv_sem=part_sems.at[w],
                device_id=peer,
                device_id_type=MESH,
            ).start()

    def rows_copy(w, j, tp, peer, recv):
        return pltpu.make_async_remote_copy(
            src_ref=residual_ref.at[w],
            dst_ref=rows_ref.at[w, j, tp],
            send_sem=sent_sems.at[1],
            recv_sem=recv,
            device_id=peer,
            device_id_type=MESH,
        )

    def spread_rows(w):
        attention = part_ref[w, my_tp].astype(f32)
        if tp_peers:
            landed = part_in_ref.at[w]
            pltpu.make_async_copy(landed, landed, part_sems.at[w]).wait()
            for i in range(len(tp_peers)):
                attention += part_in_ref[w, i].astype(f32)
        mine = tokens_ref[:, own_columns].astype(f32)[w * wave : (w + 1) * wave]
        residual_ref[w] = (mine + attention).astype(bf16)
        for i, dy in far_first:
            core, j = i // held, i % held
            peer = device(*slots[i], dy, core)
            copy = rows_copy(w, j, my_tp, peer, rows_sems.at[w, j, dy, my_core])
            if (i, dy) == (0, 0):
                pl.when(jnp.logical_not(is_home))(copy.start)
            else:
                copy.start()

        @pl.when(is_home)
        def _():
            rows_ref[w, 0, my_tp] = residual_ref[w]

    sources = [[(dy, core)] for core in range(n_core)[::-1] for dy in range(n_y)]

    def experts(w):
        squares = jnp.zeros((held * wave, 1), f32)
        for step, some in enumerate(sources):
            for dy, core in some:
                tp = device(0, 0, n_y - dy, core)[1]
                for j in range(held):
                    copy = rows_copy(w, j, tp, (my_ep, my_tp), rows_sems.at[w, j, dy, core])
                    if (j, dy, core) == (0, 0, 0):
                        pl.when(jnp.logical_not(is_home))(copy.wait_recv)
                    else:
                        copy.wait_recv()
            if (w, step) == (0, 0):
                for load in loads[12:14]:
                    load.wait()
                for copy in lent[:4]:
                    copy.wait_recv()
            scaled = []
            for dy, core in some:
                tp = device(0, 0, n_y - dy, core)[1]
                rows = jnp.concatenate(
                    [rows_ref[w, j, tp].astype(f32) for j in range(held)], axis=0
                )
                squares = squares + jnp.sum(rows * rows, axis=-1, keepdims=True)
                scaled.append((tp, (rows * ffn_gain_ref[:, column_block(tp)]).astype(bf16)))
            for k in range(n_core):
                for n, weight_ref in enumerate((w_gate_ref, w_up_ref)):
                    share = sum(dot(rows, weight_ref[k, column_block(tp), :]) for tp, rows in scaled)
                    if step:
                        share = share + hidden_ref[k, n]
                    hidden_ref[k, n] = share
        scale = lax.rsqrt(squares / model_width + epsilon)
        activated = []
        for k in range(n_core):
            gate_value = jnp.minimum(hidden_ref[k, 0] * scale, clamp_limit)
            up_value = jnp.clip(hidden_ref[k, 1] * scale, -clamp_limit, clamp_limit)
            activated.append(
                (
                    (up_value + 1.0) * gate_value * jax.nn.sigmoid(sigmoid_slope * gate_value)
                ).astype(bf16)
            )
        if w == 0:
            loads[14].wait()
            for copy in lent[4:]:
                copy.wait_recv()
        for dy in far_y:
            for core in range(n_core):
                columns = column_block(device(0, 0, dy, core)[1])
                share = sum(dot(activated[k], w_down_ref[k, :, columns]) for k in range(n_core))
                for j in range(held):
                    back_ref[w, dy, core, j] = share[j * wave : (j + 1) * wave].astype(bf16)
            for j in range(held)[::-1]:
                dz, dx = my_offset(j)
                place = j + held * my_core
                for core in range(n_core):
                    copy = pltpu.make_async_remote_copy(
                        src_ref=back_ref.at[w, dy, core, j],
                        dst_ref=back_in_ref.at[w, dy, place],
                        send_sem=sent_sems.at[2],
                        recv_sem=back_sems.at[w, place, dy],
                        device_id=device(n_z - dz, n_x - dx, dy, core),
                        device_id_type=MESH,
                    )
                    if (j, dy, core) == (0, 0, 0):
                        pl.when(jnp.logical_not(is_home))(copy.start)
                    else:
                        copy.start()

        @pl.when(is_home)
        def _():
            back_in_ref[w, 0, 0] = back_ref[w, 0, 0, 0]

    def collect(w, weights):
        total = residual_ref[w].astype(f32)
        for i in range(n_ep):
            summed = 0.0
            for dy in far_y:
                arrived = back_in_ref.at[w, dy, i]
                copy = pltpu.make_async_copy(arrived, arrived, back_sems.at[w, i, dy])
                if (i, dy) == (0, 0):
                    pl.when(jnp.logical_not(is_home))(copy.wait)
                else:
                    copy.wait()
                summed = summed + back_in_ref[w, dy, i].astype(f32)
            weight = weights[i][w * wave : (w + 1) * wave]
            total += weight * summed.astype(bf16).astype(f32)
        return total

    own_mix = share_weights(0)
    if enter_chunk == key_chunks:
        enter()
    start_bulk(loads[12:])
    heads_out = mix_values(0, own_mix, lambda: None)
    loads[11].wait()
    project(0, heads_out)
    lend(1)
    own_mix = share_weights(1)
    heads_out = mix_values(1, own_mix, lambda: spread_rows(0))
    project(1, heads_out)
    lend(2)
    spread_rows(1)
    lend(3)
    weights = []
    for i in range(n_ep):
        named = jnp.where(routes_ref[...] == device(*slots[i], 0, 0)[0], route_weights_ref[...], 0.0)
        weights.append(to_column(jnp.sum(named, axis=0, keepdims=True)))
    experts(0)
    experts(1)
    total = jnp.concatenate([collect(w, weights) for w in range(waves)], axis=0)
    out_ref[...] = total.astype(bf16)

    if tp_peers:
        pltpu.make_async_copy(part_in_ref, part_in_ref, sent_sems.at[0]).wait()
    for copy in lent:
        copy.wait_send()
    for sem in (sent_sems.at[1], sent_sems.at[2]):
        for w in range(waves):
            fewer = back_in_ref.at[w, 0, pl.ds(0, n_ep - 1)]
            for dy in range(1, n_y):
                pltpu.make_async_copy(back_in_ref.at[w, dy], back_in_ref.at[w, dy], sem).wait()

            @pl.when(is_home)
            def _():
                pltpu.make_async_copy(fewer, fewer, sem).wait()

            @pl.when(jnp.logical_not(is_home))
            def _():
                pltpu.make_async_copy(back_in_ref.at[w, 0], back_in_ref.at[w, 0], sem).wait()


def per_device(
    tokens,
    lengths,
    key_cache,
    value_cache,
    attn_gain,
    w_query,
    w_key,
    w_value,
    mix_lambda,
    head_gain,
    w_out,
    ffn_gain,
    w_gate,
    w_up,
    w_down,
    routes,
    route_weights,
):
    n_ep, n_tp = lax.axis_size("ep"), lax.axis_size("tp")
    seq_dev, model_width = tokens.shape
    cache_len, group_heads, head_width = key_cache.shape[1:]
    flat_len = cache_len * group_heads
    wave = seq_dev // waves
    wave_rows = group_heads * wave
    block = model_width // n_tp
    n_core = 2 if n_tp % 2 == 0 and n_ep % 2 == 0 else 1
    n_y = n_tp // n_core
    n_x = 2 ** ((n_ep.bit_length() - 1) // 2)
    n_x = n_x if n_ep % n_x == 0 else 1
    operands = (
        lengths.reshape(1, seq_dev),
        mix_lambda.reshape(1, group_heads),
        tokens,
        attn_gain.reshape(1, model_width),
        head_gain.reshape(1, head_width),
        ffn_gain.reshape(1, model_width),
        routes.T,
        route_weights.T,
        w_query.reshape(model_width * group_heads, head_width),
        w_key.reshape(model_width * group_heads, head_width),
        w_value.reshape(model_width * group_heads, head_width),
        key_cache.reshape(seq_dev, flat_len, head_width),
        value_cache.reshape(seq_dev, flat_len, head_width),
        w_out.reshape(group_heads * head_width, model_width),
        w_gate[0],
        w_up[0],
        w_down[0],
    )
    vmem = pltpu.VMEM
    return pl.pallas_call(
        functools.partial(layer_kernel, n_ep, n_tp, n_x, group_heads),
        out_shape=pltpu.VMEM((seq_dev, block), bf16),
        in_specs=[pl.BlockSpec(memory_space=pltpu.HBM)] * len(operands),
        out_specs=pl.BlockSpec(memory_space=vmem),
        scratch_shapes=[vmem(operand.shape, operand.dtype) for operand in operands[:-3]]
        + [vmem((n_core, *operand.shape), operand.dtype) for operand in operands[-3:]]
        + [
            vmem((waves, 2 * wave_rows, wave * head_width), bf16),
            vmem((waves, 2 * wave_rows, flat_len), f32),
            vmem((waves, wave_rows, flat_len), bf16),
            vmem((waves, n_tp, wave, block), bf16),
            vmem((waves, max(n_tp - 1, 1), wave, block), bf16),
            vmem((waves, wave, block), bf16),
            vmem((waves, n_ep // n_core, n_tp, wave, block), bf16),
            vmem((n_core, 2, n_ep // n_core * wave, w_gate.shape[2]), f32),
            vmem((waves, n_y, n_core, n_ep // n_core, wave, block), bf16),
            vmem((waves, n_y, n_ep, wave, block), bf16),
            pltpu.SemaphoreType.DMA((15,)),
            pltpu.SemaphoreType.DMA((waves, key_chunks)),
            pltpu.SemaphoreType.DMA((waves, value_chunks)),
            pltpu.SemaphoreType.DMA((2, 6)),
            pltpu.SemaphoreType.DMA((waves,)),
            pltpu.SemaphoreType.DMA((waves, n_ep // n_core, n_y, n_core)),
            pltpu.SemaphoreType.DMA((waves, n_ep, n_y)),
            pltpu.SemaphoreType.DMA((3,)),
        ],
        compiler_params=pltpu.CompilerParams(
            collective_id=0, has_side_effects=True, vmem_limit_bytes=58 * 2**20
        ),
    )(*operands)


def solution(mesh):
    placed = (
        P("ep", None),
        P("ep"),
        P("ep", None, "tp", None),
        P("ep", None, "tp", None),
        P(),
        P(None, "tp", None),
        P(None, "tp", None),
        P(None, "tp", None),
        P("tp"),
        P(),
        P("tp", None, None),
        P(),
        P("ep", None, "tp"),
        P("ep", None, "tp"),
        P("ep", "tp", None),
        P("ep", None),
        P("ep", None),
    )
    return jax.shard_map(
        per_device, mesh=mesh, in_specs=placed, out_specs=P("ep", "tp"), check_vma=False
    )
```

```python
import functools

import jax
import jax.numpy as jnp
from jax import lax
from jax.experimental import pallas as pl
from jax.experimental.pallas import tpu as pltpu
from jax.sharding import PartitionSpec as P

epsilon = 1e-06
clamp_limit = 7.0
sigmoid_slope = 1.702
branch_scale = 0.2
MESH = pl.DeviceIdType.MESH
f32, bf16 = jnp.float32, jnp.bfloat16
lane_tile = 128
wide_tile = 256
waves = 2
enter_chunk = 1
lend_from = (0, 2, 4, 6, 6)
key_chunks = 2
value_chunks = 2


def norm_rows(wide, gain):
    return wide * lax.rsqrt(jnp.mean(wide * wide, axis=-1, keepdims=True) + epsilon) * gain


def dot(left, right):
    return jnp.dot(left, right, preferred_element_type=f32)


def dot_rows(left, right):
    return lax.dot_general(left, right, (((1,), (1,)), ((), ())), preferred_element_type=f32)


def iota(shape, axis):
    return lax.broadcasted_iota(jnp.int32, shape, axis)


def to_column(row):
    size = row.shape[1]
    eye = iota((size, size), 0) == iota((size, size), 1)
    return jnp.sum(jnp.where(eye, row, jnp.zeros_like(row)), axis=1, keepdims=True)


def layer_kernel(
    n_ep,
    n_tp,
    n_x,
    group_heads,
    lengths_hbm,
    lambda_hbm,
    tokens_hbm,
    attn_gain_hbm,
    head_gain_hbm,
    ffn_gain_hbm,
    routes_hbm,
    route_weights_hbm,
    w_query_hbm,
    w_key_hbm,
    w_value_hbm,
    key_hbm,
    value_hbm,
    w_out_hbm,
    w_gate_hbm,
    w_up_hbm,
    w_down_hbm,
    out_ref,
    lengths_ref,
    lambda_ref,
    tokens_ref,
    attn_gain_ref,
    head_gain_ref,
    ffn_gain_ref,
    routes_ref,
    route_weights_ref,
    w_query_ref,
    w_key_ref,
    w_value_ref,
    key_ref,
    value_ref,
    w_out_ref,
    w_gate_ref,
    w_up_ref,
    w_down_ref,
    query_ref,
    score_ref,
    mix_ref,
    part_ref,
    part_in_ref,
    residual_ref,
    rows_ref,
    hidden_ref,
    back_ref,
    back_in_ref,
    load_sems,
    key_sems,
    value_sems,
    lent_sems,
    part_sems,
    rows_sems,
    back_sems,
    sent_sems,
):
    my_ep, my_tp = lax.axis_index("ep"), lax.axis_index("tp")
    n_core = 2 if n_tp % 2 == 0 and n_ep % 2 == 0 else 1
    n_y = n_tp // n_core
    n_z = n_ep // n_x
    my_y, my_core = my_tp // n_core, lax.rem(my_tp, n_core)
    my_z, my_x = my_ep // n_x, lax.rem(my_ep, n_x)
    seq_dev, model_width = tokens_ref.shape
    flat_len, head_width = key_ref.shape[1:]
    half_width = head_width // 2
    block = out_ref.shape[1]

    singles = (
        (tokens_hbm, tokens_ref),
        (attn_gain_hbm, attn_gain_ref),
        (w_query_hbm, w_query_ref),
        (w_key_hbm, w_key_ref),
        (w_value_hbm, w_value_ref),
        (lengths_hbm, lengths_ref),
        (lambda_hbm, lambda_ref),
        (head_gain_hbm, head_gain_ref),
        (ffn_gain_hbm, ffn_gain_ref),
        (routes_hbm, routes_ref),
        (route_weights_hbm, route_weights_ref),
        (w_out_hbm, w_out_ref),
        (w_gate_hbm, w_gate_ref.at[0]),
        (w_up_hbm, w_up_ref.at[0]),
        (w_down_hbm, w_down_ref.at[0]),
    )
    loads = [
        pltpu.make_async_copy(source, target, load_sems.at[i])
        for i, (source, target) in enumerate(singles)
    ]
    chunk = flat_len // key_chunks
    wave = seq_dev // waves
    value_group = wave // value_chunks
    key_loads = [
        [
            pltpu.make_async_copy(
                key_hbm.at[pl.ds(w * wave, wave), pl.ds(j * chunk, chunk), :],
                key_ref.at[pl.ds(w * wave, wave), pl.ds(j * chunk, chunk), :],
                key_sems.at[w, j],
            )
            for j in range(key_chunks)
        ]
        for w in range(waves)
    ]
    value_loads = [
        [
            pltpu.make_async_copy(
                value_hbm.at[pl.ds(w * wave + i * value_group, value_group)],
                value_ref.at[pl.ds(w * wave + i * value_group, value_group)],
                value_sems.at[w, i],
            )
            for i in range(value_chunks)
        ]
        for w in range(waves)
    ]

    def start_bulk(copies):
        for copy in copies:
            copy.start(priority=1)

    for copy in loads[:11]:
        copy.start()
    start_bulk(key_loads[0])

    def device(dz, dx, dy, core):
        ep = lax.rem(my_z + dz, n_z) * n_x + lax.rem(my_x + dx, n_x)
        return ep, lax.rem(my_y + dy, n_y) * n_core + core

    def hops(offset):
        dz, dx = offset
        return min(dz, n_z - dz) + min(dx, n_x - dx)

    slots = sorted([(dz, dx) for dz in range(n_z) for dx in range(n_x)], key=hops)
    held = n_ep // n_core
    far_y = sorted(range(n_y), key=lambda dy: -min(dy, n_y - dy))
    far_first = [(i, dy) for i in range(n_ep)[::-1] for dy in far_y]
    tp_peers = [(dy, dc) for dy in range(n_y) for dc in range(n_core)][1:]
    sibling_core = lax.rem(my_core + 1, n_core)

    def my_offset(j):
        dz, dx = slots[j]
        for core in range(1, n_core):
            next_z, next_x = slots[j + core * held]
            last_z, last_x = slots[j + (core - 1) * held]
            past = (my_core + n_core - core) // n_core
            dz, dx = dz + (next_z - last_z) * past, dx + (next_x - last_x) * past
        return dz, dx

    barrier = pltpu.get_barrier_semaphore()

    def greet(peer):
        pl.semaphore_signal(barrier, inc=1, device_id=peer, device_id_type=MESH)

    for i, dy in far_first[:-1]:
        for core in range(n_core):
            greet(device(*slots[i], dy, core))
    for dc in range(1, n_core):
        greet(device(0, 0, 0, lax.rem(my_core + dc, n_core)))
    greeted = n_ep * n_tp - 1

    loads[0].wait()
    loads[1].wait()
    start_bulk(value_loads[0])
    normed = norm_rows(tokens_ref[...].astype(f32), attn_gain_ref[...]).astype(bf16)
    span = wide_tile * group_heads
    blocks = model_width // wide_tile
    stacked = jnp.concatenate(
        [normed[:, b * wide_tile : (b + 1) * wide_tile] for b in range(blocks)], axis=0
    )
    if group_heads > 1:
        spread = iota((wide_tile, span), 1) // group_heads == iota((wide_tile, span), 0)
        stacked = dot(stacked, spread.astype(f32).astype(bf16))
    else:
        stacked = stacked.astype(f32)
    lane_head = lax.rem(iota((1, span), 1), group_heads)
    left = jnp.concatenate(
        [
            jnp.concatenate(
                [
                    jnp.where(
                        lane_head == h, stacked[b * seq_dev : (b + 1) * seq_dev], 0.0
                    ).astype(bf16)
                    for h in range(group_heads)
                ],
                axis=0,
            )
            for b in range(blocks)
        ],
        axis=1,
    )
    loads[2].wait()
    queries = dot(left, w_query_ref[...]).astype(bf16).astype(f32)
    loads[3].wait()
    key_new = dot(left, w_key_ref[...]).astype(bf16).astype(f32)
    loads[4].wait()
    value_new = dot(left, w_value_ref[...]).astype(bf16).astype(f32)
    start_bulk(key_loads[1])

    score_scale = half_width ** (-0.5)
    first_half = iota((1, head_width), 1) < half_width
    halves = jnp.concatenate(
        [jnp.where(first_half, queries, 0.0), jnp.where(first_half, 0.0, queries)], axis=0
    )
    own = jnp.sum(halves * jnp.concatenate([key_new, key_new], axis=0), axis=-1, keepdims=True)
    own = own * score_scale
    for load in loads[5:11]:
        load.wait()
    limit = to_column(lengths_ref[...]) * group_heads
    limit = jnp.concatenate([limit] * (2 * group_heads), axis=0)
    balance = jnp.concatenate(
        [jnp.broadcast_to(lambda_ref[0:1, h : h + 1], (wave, 1)) for h in range(group_heads)],
        axis=0,
    )
    wave_rows = group_heads * wave
    row_seq = lax.rem(iota((2 * wave_rows, 1), 0), wave)
    row_head = lax.rem(iota((2 * wave_rows, 1), 0) // wave, group_heads)

    def of_wave(rows, w):
        first = range(w * wave, rows.shape[0], seq_dev)
        return jnp.concatenate([rows[r : r + wave] for r in first], axis=0)

    def pieces(source, target):
        depth = source.shape[0] // 2
        return [
            (source.at[pl.ds(first, depth)], target.at[n_core - 1, pl.ds(first, depth)])
            for first in (0, depth)
        ]

    lent = [
        pltpu.make_async_remote_copy(
            src_ref=source,
            dst_ref=target,
            send_sem=lent_sems.at[0, i],
            recv_sem=lent_sems.at[1, i],
            device_id=device(0, 0, 0, sibling_core),
            device_id_type=MESH,
        )
        for i, (source, target) in enumerate(
            pieces(w_gate_hbm, w_gate_ref)
            + pieces(w_up_hbm, w_up_ref)
            + pieces(w_down_hbm, w_down_ref)
        )
    ]
    lent = lent if n_core > 1 else []

    def lend(point):
        for copy in lent[lend_from[point] : lend_from[point + 1]]:
            copy.start()

    def enter():
        pl.semaphore_wait(barrier, greeted)
        lend(0)

    def share_weights(w):
        limits = of_wave(limit, w)
        own_score = of_wave(own, w)
        wave_halves = of_wave(halves, w)
        for s in range(wave):
            query_ref[w, :, s * head_width : (s + 1) * head_width] = jnp.where(
                row_seq == s, wave_halves, 0.0
            ).astype(bf16)

        def masked(j):
            columns = slice(j * chunk, (j + 1) * chunk)
            column = iota((1, chunk), 1) + j * chunk
            live = (column < limits) & (lax.rem(column, group_heads) == row_head)
            scores = jnp.where(live, score_ref[w, :, columns] * score_scale, -jnp.inf)
            score_ref[w, :, columns] = scores
            return jnp.max(scores, axis=-1, keepdims=True)

        peak = own_score
        for j in range(key_chunks):
            if (w, j) == (0, enter_chunk):
                enter()
            key_loads[w][j].wait()
            if (w, j) == (0, 0):
                loads[11].start()
                start_bulk(value_loads[1])
            keys = jnp.concatenate(
                [
                    key_ref[w * wave + s, j * chunk : (j + 1) * chunk, :]
                    for s in range(wave)
                ],
                axis=1,
            )
            score_ref[w, :, j * chunk : (j + 1) * chunk] = dot_rows(query_ref[w], keys)
            if j:
                peak = jnp.maximum(peak, masked(j - 1))
        peak = jnp.maximum(peak, masked(key_chunks - 1))
        own_weight = jnp.exp(own_score - peak)
        denominator = own_weight
        for j in range(key_chunks):
            columns = slice(j * chunk, (j + 1) * chunk)
            weights = jnp.exp(score_ref[w, :, columns] - peak)
            score_ref[w, :, columns] = weights
            denominator = denominator + jnp.sum(weights, axis=-1, keepdims=True)
        inverse = 1.0 / denominator
        own_share = own_weight * inverse
        own_mix = own_share[:wave_rows] - balance * own_share[wave_rows:]
        minuend, subtrahend = inverse[:wave_rows], balance * inverse[wave_rows:]
        for j in range(key_chunks):
            columns = slice(j * chunk, (j + 1) * chunk)
            mix_ref[w, :, columns] = (
                score_ref[w, :wave_rows, columns] * minuend
                - score_ref[w, wave_rows:, columns] * subtrahend
            ).astype(bf16)
        return own_mix.astype(bf16).astype(f32)

    def mix_values(w, own_mix, before_last):
        heads_out = own_mix * of_wave(value_new, w)
        for i in range(value_chunks):
            if i == value_chunks - 1:
                before_last()
            value_loads[w][i].wait()
            members = range(i * value_group, (i + 1) * value_group)
            values = jnp.concatenate([value_ref[w * wave + s] for s in members], axis=1)
            mixed = dot(mix_ref[w], values)
            for k, s in enumerate(members):
                heads_out = heads_out + jnp.where(
                    row_seq[:wave_rows] == s, mixed[:, k * head_width : (k + 1) * head_width], 0.0
                )
        return heads_out

    def column_block(tp):
        return pl.ds(pl.multiple_of(tp * block, block), block)

    is_home = my_core == 0
    own_columns = column_block(my_tp)

    def project(w, heads_out):
        heads = norm_rows(heads_out, head_gain_ref[...] * branch_scale)
        heads = jnp.concatenate(
            [heads[h * wave : (h + 1) * wave] for h in range(group_heads)], axis=1
        ).astype(bf16)
        for t in range(n_tp):
            part_ref[w, t] = dot(heads, w_out_ref[:, t * block : (t + 1) * block]).astype(bf16)
        for i, (dy, dc) in enumerate(tp_peers):
            peer = device(0, 0, dy, lax.rem(my_core + dc, n_core))
            pltpu.make_async_remote_copy(
                src_ref=part_ref.at[w, peer[1]],
                dst_ref=part_in_ref.at[w, i],
                send_sem=sent_sems.at[0],
                recv_sem=part_sems.at[w],
                device_id=peer,
                device_id_type=MESH,
            ).start()

    def rows_copy(w, j, tp, peer, recv):
        return pltpu.make_async_remote_copy(
            src_ref=residual_ref.at[w],
            dst_ref=rows_ref.at[w, j, tp],
            send_sem=sent_sems.at[1],
            recv_sem=recv,
            device_id=peer,
            device_id_type=MESH,
        )

    def spread_rows(w):
        attention = part_ref[w, my_tp].astype(f32)
        if tp_peers:
            landed = part_in_ref.at[w]
            pltpu.make_async_copy(landed, landed, part_sems.at[w]).wait()
            for i in range(len(tp_peers)):
                attention += part_in_ref[w, i].astype(f32)
        mine = tokens_ref[:, own_columns].astype(f32)[w * wave : (w + 1) * wave]
        residual_ref[w] = (mine + attention).astype(bf16)
        for i, dy in far_first:
            core, j = i // held, i % held
            peer = device(*slots[i], dy, core)
            copy = rows_copy(w, j, my_tp, peer, rows_sems.at[w, j, dy, my_core])
            if (i, dy) == (0, 0):
                pl.when(jnp.logical_not(is_home))(copy.start)
            else:
                copy.start()

        @pl.when(is_home)
        def _():
            rows_ref[w, 0, my_tp] = residual_ref[w]

    sources = [[(dy, core)] for core in range(n_core)[::-1] for dy in range(n_y)]

    def experts(w):
        squares = jnp.zeros((held * wave, 1), f32)
        for step, some in enumerate(sources):
            for dy, core in some:
                tp = device(0, 0, n_y - dy, core)[1]
                for j in range(held):
                    copy = rows_copy(w, j, tp, (my_ep, my_tp), rows_sems.at[w, j, dy, core])
                    if (j, dy, core) == (0, 0, 0):
                        pl.when(jnp.logical_not(is_home))(copy.wait_recv)
                    else:
                        copy.wait_recv()
            if (w, step) == (0, 0):
                for load in loads[12:14]:
                    load.wait()
                for copy in lent[:4]:
                    copy.wait_recv()
            scaled = []
            for dy, core in some:
                tp = device(0, 0, n_y - dy, core)[1]
                rows = jnp.concatenate(
                    [rows_ref[w, j, tp].astype(f32) for j in range(held)], axis=0
                )
                squares = squares + jnp.sum(rows * rows, axis=-1, keepdims=True)
                scaled.append((tp, (rows * ffn_gain_ref[:, column_block(tp)]).astype(bf16)))
            for k in range(n_core):
                for n, weight_ref in enumerate((w_gate_ref, w_up_ref)):
                    share = sum(dot(rows, weight_ref[k, column_block(tp), :]) for tp, rows in scaled)
                    if step:
                        share = share + hidden_ref[k, n]
                    hidden_ref[k, n] = share
        scale = lax.rsqrt(squares / model_width + epsilon)
        activated = []
        for k in range(n_core):
            gate_value = jnp.minimum(hidden_ref[k, 0] * scale, clamp_limit)
            up_value = jnp.clip(hidden_ref[k, 1] * scale, -clamp_limit, clamp_limit)
            activated.append(
                (
                    (up_value + 1.0) * gate_value * jax.nn.sigmoid(sigmoid_slope * gate_value)
                ).astype(bf16)
            )
        if w == 0:
            loads[14].wait()
            for copy in lent[4:]:
                copy.wait_recv()
        returned = {}
        for dy in far_y:
            for core in range(n_core):
                columns = column_block(device(0, 0, dy, core)[1])
                returned[dy, core] = sum(
                    dot(activated[k], w_down_ref[k, :, columns]) for k in range(n_core)
                )
        for dy in far_y:
            for core in range(n_core):
                for j in range(held):
                    back_ref[w, dy, core, j] = returned[dy, core][
                        j * wave : (j + 1) * wave
                    ].astype(bf16)
            for j in range(held)[::-1]:
                dz, dx = my_offset(j)
                place = j + held * my_core
                for core in range(n_core):
                    copy = pltpu.make_async_remote_copy(
                        src_ref=back_ref.at[w, dy, core, j],
                        dst_ref=back_in_ref.at[w, dy, place],
                        send_sem=sent_sems.at[2],
                        recv_sem=back_sems.at[w, place, dy],
                        device_id=device(n_z - dz, n_x - dx, dy, core),
                        device_id_type=MESH,
                    )
                    if (j, dy, core) == (0, 0, 0):
                        pl.when(jnp.logical_not(is_home))(copy.start)
                    else:
                        copy.start()

        @pl.when(is_home)
        def _():
            back_in_ref[w, 0, 0] = back_ref[w, 0, 0, 0]

    def collect(w, weights):
        total = residual_ref[w].astype(f32)
        for i in range(n_ep):
            summed = 0.0
            for dy in far_y:
                arrived = back_in_ref.at[w, dy, i]
                copy = pltpu.make_async_copy(arrived, arrived, back_sems.at[w, i, dy])
                if (i, dy) == (0, 0):
                    pl.when(jnp.logical_not(is_home))(copy.wait)
                else:
                    copy.wait()
                summed = summed + back_in_ref[w, dy, i].astype(f32)
            weight = weights[i][w * wave : (w + 1) * wave]
            total += weight * summed.astype(bf16).astype(f32)
        return total

    own_mix = share_weights(0)
    if enter_chunk == key_chunks:
        enter()
    start_bulk(loads[12:])
    heads_out = mix_values(0, own_mix, lambda: None)
    loads[11].wait()
    project(0, heads_out)
    lend(1)
    own_mix = share_weights(1)
    heads_out = mix_values(1, own_mix, lambda: spread_rows(0))
    project(1, heads_out)
    lend(2)
    spread_rows(1)
    lend(3)
    weights = []
    for i in range(n_ep):
        named = jnp.where(routes_ref[...] == device(*slots[i], 0, 0)[0], route_weights_ref[...], 0.0)
        weights.append(to_column(jnp.sum(named, axis=0, keepdims=True)))
    experts(0)
    experts(1)
    total = jnp.concatenate([collect(w, weights) for w in range(waves)], axis=0)
    out_ref[...] = total.astype(bf16)

    if tp_peers:
        pltpu.make_async_copy(part_in_ref, part_in_ref, sent_sems.at[0]).wait()
    for copy in lent:
        copy.wait_send()
    for sem in (sent_sems.at[1], sent_sems.at[2]):
        for w in range(waves):
            fewer = back_in_ref.at[w, 0, pl.ds(0, n_ep - 1)]
            for dy in range(1, n_y):
                pltpu.make_async_copy(back_in_ref.at[w, dy], back_in_ref.at[w, dy], sem).wait()

            @pl.when(is_home)
            def _():
                pltpu.make_async_copy(fewer, fewer, sem).wait()

            @pl.when(jnp.logical_not(is_home))
            def _():
                pltpu.make_async_copy(back_in_ref.at[w, 0], back_in_ref.at[w, 0], sem).wait()


def per_device(
    tokens,
    lengths,
    key_cache,
    value_cache,
    attn_gain,
    w_query,
    w_key,
    w_value,
    mix_lambda,
    head_gain,
    w_out,
    ffn_gain,
    w_gate,
    w_up,
    w_down,
    routes,
    route_weights,
):
    n_ep, n_tp = lax.axis_size("ep"), lax.axis_size("tp")
    seq_dev, model_width = tokens.shape
    cache_len, group_heads, head_width = key_cache.shape[1:]
    flat_len = cache_len * group_heads
    wave = seq_dev // waves
    wave_rows = group_heads * wave
    block = model_width // n_tp
    n_core = 2 if n_tp % 2 == 0 and n_ep % 2 == 0 else 1
    n_y = n_tp // n_core
    n_x = 2 ** ((n_ep.bit_length() - 1) // 2)
    n_x = n_x if n_ep % n_x == 0 else 1
    operands = (
        lengths.reshape(1, seq_dev),
        mix_lambda.reshape(1, group_heads),
        tokens,
        attn_gain.reshape(1, model_width),
        head_gain.reshape(1, head_width),
        ffn_gain.reshape(1, model_width),
        routes.T,
        route_weights.T,
        w_query.reshape(model_width * group_heads, head_width),
        w_key.reshape(model_width * group_heads, head_width),
        w_value.reshape(model_width * group_heads, head_width),
        key_cache.reshape(seq_dev, flat_len, head_width),
        value_cache.reshape(seq_dev, flat_len, head_width),
        w_out.reshape(group_heads * head_width, model_width),
        w_gate[0],
        w_up[0],
        w_down[0],
    )
    vmem = pltpu.VMEM
    return pl.pallas_call(
        functools.partial(layer_kernel, n_ep, n_tp, n_x, group_heads),
        out_shape=pltpu.VMEM((seq_dev, block), bf16),
        in_specs=[pl.BlockSpec(memory_space=pltpu.HBM)] * len(operands),
        out_specs=pl.BlockSpec(memory_space=vmem),
        scratch_shapes=[vmem(operand.shape, operand.dtype) for operand in operands[:-3]]
        + [vmem((n_core, *operand.shape), operand.dtype) for operand in operands[-3:]]
        + [
            vmem((waves, 2 * wave_rows, wave * head_width), bf16),
            vmem((waves, 2 * wave_rows, flat_len), f32),
            vmem((waves, wave_rows, flat_len), bf16),
            vmem((waves, n_tp, wave, block), bf16),
            vmem((waves, max(n_tp - 1, 1), wave, block), bf16),
            vmem((waves, wave, block), bf16),
            vmem((waves, n_ep // n_core, n_tp, wave, block), bf16),
            vmem((n_core, 2, n_ep // n_core * wave, w_gate.shape[2]), f32),
            vmem((waves, n_y, n_core, n_ep // n_core, wave, block), bf16),
            vmem((waves, n_y, n_ep, wave, block), bf16),
            pltpu.SemaphoreType.DMA((15,)),
            pltpu.SemaphoreType.DMA((waves, key_chunks)),
            pltpu.SemaphoreType.DMA((waves, value_chunks)),
            pltpu.SemaphoreType.DMA((2, 6)),
            pltpu.SemaphoreType.DMA((waves,)),
            pltpu.SemaphoreType.DMA((waves, n_ep // n_core, n_y, n_core)),
            pltpu.SemaphoreType.DMA((waves, n_ep, n_y)),
            pltpu.SemaphoreType.DMA((3,)),
        ],
        compiler_params=pltpu.CompilerParams(
            collective_id=0, has_side_effects=True, vmem_limit_bytes=58 * 2**20
        ),
    )(*operands)


def solution(mesh):
    placed = (
        P("ep", None),
        P("ep"),
        P("ep", None, "tp", None),
        P("ep", None, "tp", None),
        P(),
        P(None, "tp", None),
        P(None, "tp", None),
        P(None, "tp", None),
        P("tp"),
        P(),
        P("tp", None, None),
        P(),
        P("ep", None, "tp"),
        P("ep", None, "tp"),
        P("ep", "tp", None),
        P("ep", None),
        P("ep", None),
    )
    return jax.shard_map(
        per_device, mesh=mesh, in_specs=placed, out_specs=P("ep", "tp"), check_vma=False
    )
```
